32 devices in a mesh: sp: 8 (over z, y), tp: 4 (over x, core).
Axes of the slice: x: 2, y: 2, z: 4, core: 2. Of those that a mesh axis runs over, the one named last changes fastest.
Arguments:
- tokens: bfloat16 [8192, 4096], P('sp', 'tp'), may hold values from -6 to 6
- norm_gain: float32 [4096], replicated, may hold values from 0.1 to 1.9
- pool_in_weight: bfloat16 [4096, 2048], P('sp', 'tp'), may hold values from -0.09375 to 0.09375
- query_weight: bfloat16 [4096, 2048], P('sp', 'tp'), may hold values from -1 to 1, as said below
- key_weight: bfloat16 [4096, 512], P('sp', 'tp'), may hold values from -40 to 40
- value_weight: bfloat16 [4096, 512], P('sp', 'tp'), may hold values from -0.09375 to 0.09375
- pool_weight: bfloat16 [8, 256, 256], P('tp'), may hold values from -0.375 to 0.375
- pool_scale: float32 [2048], P('tp'), may hold values from 0.1 to 1.9
- sink_logit: float32 [32], P('tp'), may hold values from 3 to 7
- out_pool_weight: bfloat16 [2048, 4096], P('tp', 'sp'), may hold values from -0.09375 to 0.09375
- out_attn_weight: bfloat16 [2048, 4096], P('tp', 'sp'), may hold values from -1.5 to 1.5
Outputs:
- mixed: bfloat16 [8192, 4096], P(('sp', 'tp'))
The draws below stay inside these ranges and needn't reach their ends.
Inputs may be any that keep to these rules, and one draw needn't show every extreme that they name: `query_weight`: entries of order 4096 ** -0.5, drawn independently.
All inputs are finite; a program needn't handle non-finite values.
Results may differ from the reference program's by a relative error of at most 0.014.
The reference program's roundings to bfloat16 on the way count: a program that leaves them out, or rounds other values in their place, can miss the bound.
Values may be sent and summed in bfloat16 or wider, within the bound.
A program may use at most 128 MiB of HBM per device.

```python
import jax
import jax.numpy as jnp
from jax import lax

D = 4096
HEAD_DIM = 64
Q_HEADS = 32
KV_HEADS = 8
POOL_GROUPS = 8
GROUP_DIM = 256
WINDOW = 128
GRID_W = 64
TOK_DEV = 1024
TOKENS = 8192
POOL_WIDTH = 2048
ATTN_WIDTH = 2048
KV_WIDTH = 512
N_TP = 4


def weight_pair(key):
    query_part = jax.random.normal(jax.random.fold_in(key, 11), (D, ATTN_WIDTH), jnp.float32) * D ** (-0.5)
    key_part = jax.random.normal(jax.random.fold_in(key, 12), (D, KV_WIDTH), jnp.float32) * D ** (-0.5)
    return (query_part, key_part)


def draw_query_weight(key, part):
    return weight_pair(key)[0].astype(jnp.bfloat16)


def draw_key_weight(key, part):
    query_part, key_part = weight_pair(key)
    return key_part.astype(jnp.bfloat16)


def shard_levels(key, extent, pieces, smallest, high):
    level, own = 1.0, jax.random.fold_in(key, 6)
    for position, shards_of in pieces:
        heights = jnp.exp(jax.random.uniform(jax.random.fold_in(own, position), (shards_of,), jnp.float32, smallest / len(pieces), high / len(pieces)))
        level = level * jnp.repeat(heights, extent[position] // shards_of).reshape([-1 if axis == position else 1 for axis in range(len(extent))])
    return level


def noise(key, dims, width, reach, cuts=(), held_as=jnp.bfloat16):
    values = jax.random.normal(key, dims, jnp.float32) * width
    if len(cuts) > 0:
        values = shard_levels(key, dims, cuts, -0.22, 0.18) * values
    return jnp.clip(values, min=-reach, max=reach).astype(held_as)


def setup_inputs(seed: int = 0) -> dict:
    seeds = jax.random.split(jax.random.key(seed), 12)
    tokens = noise(seeds[0], (TOKENS, D), 1.0, 6.0, ((0, 8), (1, 4)))
    norm_gain = jnp.clip(1.0 + 0.18 * jax.random.normal(seeds[1], (D,), jnp.float32), 0.1, 1.9)
    pool_in_weight = noise(seeds[2], (D, POOL_WIDTH), D ** -0.5, 0.09375, ((0, 8), (1, 4)))
    query_weight = draw_query_weight(jax.random.fold_in(seeds[11], 71), 0)
    key_weight = draw_key_weight(jax.random.fold_in(seeds[11], 71), 0)
    value_weight = noise(seeds[5], (D, KV_WIDTH), D ** -0.5, 0.09375, ((0, 8), (1, 4)))
    pool_weight = noise(seeds[6], (POOL_GROUPS, GROUP_DIM, GROUP_DIM), GROUP_DIM ** -0.5, 0.375, ((0, 4),))
    pool_scale = jnp.clip(1.0 + 0.18 * jax.random.normal(seeds[7], (POOL_WIDTH,), jnp.float32), 0.1, 1.9)
    sink_logit = jnp.clip(3.0 + 4.0 * jax.random.uniform(seeds[8], (Q_HEADS,), jnp.float32) ** shard_levels(seeds[8], (Q_HEADS,), ((0, 4),), -0.2, 0.2), 3.0, 7.0)
    out_pool_weight = noise(seeds[9], (POOL_WIDTH, D), (2 * POOL_WIDTH) ** -0.5, 0.09375, ((0, 4), (1, 8)))
    out_attn_weight = noise(seeds[10], (ATTN_WIDTH, D), (ATTN_WIDTH // 128) ** -0.5, 1.5, ((0, 4), (1, 8)))
    return dict(tokens=tokens, norm_gain=norm_gain, pool_in_weight=pool_in_weight, query_weight=query_weight, key_weight=key_weight, value_weight=value_weight, pool_weight=pool_weight, pool_scale=pool_scale, sink_logit=sink_logit, out_pool_weight=out_pool_weight, out_attn_weight=out_attn_weight)


epsilon = 1e-06
rotary_base = 10000.0
masked_score = -1e+30

def rms_normed(values, gain):
    floats = values.astype(jnp.float32)
    scaled = floats * lax.rsqrt(lax.optimization_barrier(jnp.mean(floats * floats, axis=-1, keepdims=True)) + epsilon)
    return (scaled * gain).astype(jnp.bfloat16)

def rotary_tables(positions, head_dim, grid_width):
    freq_count = head_dim // 4
    inverse = rotary_base ** (-jnp.arange(freq_count, dtype=jnp.float32) / freq_count)
    row_pos = (positions // grid_width).astype(jnp.float32)
    col_pos = (positions % grid_width).astype(jnp.float32)
    angles = jnp.stack([row_pos[:, None] * inverse, col_pos[:, None] * inverse], axis=1)
    return (jnp.cos(angles), jnp.sin(angles))

def rotate(values, cosine, sine):
    length, heads, head_dim = values.shape
    split = values.reshape(length, heads, 2, 2, head_dim // 4)
    first = split[:, :, :, 0]
    second = split[:, :, :, 1]
    cos_b = cosine[:, None]
    sin_b = sine[:, None]
    turned = jnp.stack([first * cos_b - second * sin_b, second * cos_b + first * sin_b], axis=3)
    return turned.reshape(length, heads, head_dim)

def pool_branch(pool_in, pool_weight, pool_scale):
    length, channels = pool_in.shape
    running = jnp.concatenate([jnp.zeros((1, channels), jnp.float32), jnp.cumsum(pool_in.astype(jnp.float32), axis=0)], axis=0)
    group_ids = jnp.arange(channels, dtype=jnp.int32) // GROUP_DIM
    halves = jnp.array([1, 2, 4, 8], jnp.int32)[group_ids % 4]
    positions = jnp.arange(length, dtype=jnp.int32)[:, None]
    lower = jnp.clip(positions - halves[None, :], 0, length).astype(jnp.int32)
    upper = jnp.clip(positions + halves[None, :], 0, length).astype(jnp.int32)
    window_sum = jnp.take_along_axis(running, upper, 0) - jnp.take_along_axis(running, lower, 0)
    window_mean = window_sum / (upper - lower).astype(jnp.float32)
    pooled = (window_mean - pool_in.astype(jnp.float32)).astype(jnp.bfloat16)
    grouped = pooled.reshape(length, channels // GROUP_DIM, GROUP_DIM).astype(jnp.float32)
    mixing = jnp.einsum('lgc,gcd->lgd', grouped, pool_weight.astype(jnp.float32))
    return (mixing.reshape(length, channels) * pool_scale).astype(jnp.bfloat16)

def attention_branch(queries, key_rows, value_rows, sink_logit, block):
    length = queries.shape[0]
    group = Q_HEADS // KV_HEADS
    pad_keys = jnp.pad(key_rows, ((WINDOW, WINDOW), (0, 0), (0, 0)))
    pad_values = jnp.pad(value_rows, ((WINDOW, WINDOW), (0, 0), (0, 0)))
    span = block + 2 * WINDOW

    def one_block(index):
        start = (index * block).astype(jnp.int32)
        query_block = lax.dynamic_slice_in_dim(queries, start, block, 0).astype(jnp.float32)
        query_block = query_block.reshape(block, KV_HEADS, group, HEAD_DIM)
        key_block = lax.dynamic_slice_in_dim(pad_keys, start, span, 0).astype(jnp.float32)
        value_block = lax.dynamic_slice_in_dim(pad_values, start, span, 0).astype(jnp.float32)
        scores = jnp.einsum('qkgd,skd->kgqs', query_block, key_block) * HEAD_DIM ** (-0.5)
        query_pos = start + jnp.arange(block, dtype=jnp.int32)
        key_pos = start - WINDOW + jnp.arange(span, dtype=jnp.int32)
        allowed = (jnp.abs(key_pos[None, :] - query_pos[:, None]) <= WINDOW) & (key_pos >= 0)[None, :] & (key_pos < length)[None, :]
        scores = jnp.where(allowed, scores, masked_score)
        sink = jnp.broadcast_to(sink_logit.reshape(KV_HEADS, group, 1, 1), scores.shape[:-1] + (1,))
        weights = jax.nn.softmax(jnp.concatenate([scores, sink], axis=-1), axis=-1)[..., :-1]
        weights = weights.astype(jnp.bfloat16).astype(jnp.float32)
        output = jnp.einsum('kgqs,skd->qkgd', weights, value_block)
        return output.reshape(block, Q_HEADS * HEAD_DIM).astype(jnp.bfloat16)
    blocks = lax.map(one_block, jnp.arange(length // block, dtype=jnp.int32))
    return blocks.reshape(length, Q_HEADS * HEAD_DIM)

def reference(tokens, norm_gain, pool_in_weight, query_weight, key_weight, value_weight, pool_weight, pool_scale, sink_logit, out_pool_weight, out_attn_weight):
    length = tokens.shape[0]
    normed = rms_normed(tokens, norm_gain)
    pool_in = jnp.dot(normed, pool_in_weight, preferred_element_type=jnp.float32).astype(jnp.bfloat16)
    positions = jnp.arange(length, dtype=jnp.int32)
    cosine, sine = rotary_tables(positions, HEAD_DIM, GRID_W)
    query_raw = jnp.dot(normed, query_weight, preferred_element_type=jnp.float32)
    queries = rotate(query_raw.reshape(length, Q_HEADS, HEAD_DIM), cosine, sine).astype(jnp.bfloat16)
    key_raw = jnp.dot(normed, key_weight, preferred_element_type=jnp.float32)
    key_rows = rotate(key_raw.reshape(length, KV_HEADS, HEAD_DIM), cosine, sine).astype(jnp.bfloat16)
    value_rows = jnp.dot(normed, value_weight, preferred_element_type=jnp.float32).astype(jnp.bfloat16)
    value_rows = value_rows.reshape(length, KV_HEADS, HEAD_DIM)
    pool_out = pool_branch(pool_in, pool_weight, pool_scale)
    attn_out = attention_branch(queries, key_rows, value_rows, sink_logit, TOK_DEV)
    pool_share = POOL_WIDTH // N_TP
    attn_share = ATTN_WIDTH // N_TP
    mixed = jnp.zeros((length, D), jnp.float32)
    for index in range(N_TP):
        partial_value = jnp.dot(pool_out[:, index * pool_share:(index + 1) * pool_share], out_pool_weight[index * pool_share:(index + 1) * pool_share], preferred_element_type=jnp.float32)
        partial_value = partial_value + jnp.dot(attn_out[:, index * attn_share:(index + 1) * attn_share], out_attn_weight[index * attn_share:(index + 1) * attn_share], preferred_element_type=jnp.float32)
        mixed = mixed + partial_value.astype(jnp.bfloat16).astype(jnp.float32)
    return mixed.astype(jnp.bfloat16)
```

```python
import functools

import jax
import jax.numpy as jnp
import numpy as np
from jax import lax
from jax.experimental import pallas as pl
from jax.experimental.pallas import tpu as pltpu
from jax.sharding import PartitionSpec as P

HEAD_DIM = 64
Q_HEADS = 32
KV_HEADS = 8
GROUP_DIM = 256
WINDOW = 128
GRID_W = 64
LANES = 128
SUBS = 4
CHUNKS = 4
POOL_PAD = 16
LAG = 5

epsilon = 1e-06
rotary_base = 10000.0
masked_score = -1e30
MESH = pl.DeviceIdType.MESH


def rotary_tables(total_rows):
    freq_count = HEAD_DIM // 4
    inverse = np.float32(rotary_base) ** (-np.arange(freq_count, dtype=np.float32) / np.float32(freq_count))
    lane = np.arange(LANES)
    dim = lane % HEAD_DIM
    by_col = (dim // (HEAD_DIM // 2)) == 1
    is_b = (dim % (HEAD_DIM // 2)) // freq_count == 1
    freq = inverse[dim % freq_count]
    sign = np.where(is_b, np.float32(1.0), np.float32(-1.0))
    tables = []
    for count, mine in ((total_rows // GRID_W, ~by_col), (GRID_W, by_col)):
        angle = np.arange(count, dtype=np.float32)[:, None] * freq[None, :]
        tables.append(np.where(mine, np.cos(angle), np.float32(0.0)).astype(np.float32))
        tables.append(np.where(mine, np.sin(angle) * sign, np.float32(0.0)).astype(np.float32))
    return tables


def spread_matrix(kv_width):
    heads = kv_width // HEAD_DIM
    spread = np.zeros((2 * kv_width, 4 * heads * LANES), np.float32)
    for kind in range(2):
        for head in range(heads):
            for half in range(2):
                block = (kind * heads + head) * 2 + half
                for d in range(HEAD_DIM):
                    spread[kind * kv_width + head * HEAD_DIM + d, block * LANES + half * HEAD_DIM + d] = 1.0
    return spread


def layer_kernel(
    dims,
    tokens,
    pool_in_w,
    query_w,
    kv_parts,
    out_pool_w,
    out_attn_w,
    gain,
    pool_w,
    pool_scale,
    sink,
    row_cos,
    row_sin,
    col_cos,
    col_sin,
    spread,
    out,
    tok,
    in_w,
    out_w,
    acc,
    queries,
    pool_pad,
    kv,
    kvx,
    mixers,
    to_core,
    own_sum,
    from_core,
    from_chip,
    load_sem,
    in_send,
    in_recv,
    ow_send,
    ow_recv,
    tx_send,
    tx_recv,
    td_send,
    td_recv,
    halo_send,
    halo_recv,
    core_send,
    core_recv,
    chip_send,
    chip_recv,
):
    n_sp, n_tp = dims["sp"], dims["tp"]
    rows, feats = tokens.shape
    depth = pool_in_w.shape[0]
    pool_ch = pool_in_w.shape[1]
    q_width = query_w.shape[1]
    kvw = dims["kvw"]
    cols_dev = out_pool_w.shape[1]
    nq = dims["nq"]
    nr = SUBS // nq
    col_q = cols_dev // nq
    half = n_sp // 2
    chips = n_tp // 2
    part_rows = rows // n_tp
    pieces = n_sp * nq

    sp = lax.axis_index("sp")
    tp = lax.axis_index("tp")
    chip = tp // 2
    core = tp % 2
    place = jnp.where(sp % 2 == 0, sp // 2, n_sp - 1 - sp // 2)

    def owner_at(spot):
        spot = (spot + n_sp) % n_sp
        return jnp.where(spot < half, 2 * spot, 2 * (n_sp - 1 - spot) + 1)

    ahead = (owner_at(place + 1), tp)
    behind = (owner_at(place - 1), tp)
    partner = (sp, chip * 2 + 1 - core)

    def chip_peer(rel):
        return (sp, ((chip + rel) % chips) * 2 + core)

    def source_slot(rel):
        return ((chip - rel + chips) % chips) * 2 + core

    barrier = pltpu.get_barrier_semaphore()
    greeted = [ahead, behind, ((sp + 1) % n_sp, tp), ((sp + n_sp - 1) % n_sp, tp), partner]
    greeted += [chip_peer(rel) for rel in range(1, chips)]
    for other in greeted:
        pl.semaphore_signal(barrier, inc=1, device_id=other, device_id_type=MESH)

    loads = []

    def load(src, dst):
        copy = pltpu.make_async_copy(src, dst, load_sem.at[len(loads)])
        copy.start()
        loads.append(copy)

    load(pool_in_w, in_w.at[sp, :, pl.ds(0, pool_ch)])
    load(query_w, in_w.at[sp, :, pl.ds(pool_ch, q_width)])
    start = pool_ch + q_width
    for part in kv_parts:
        load(part, in_w.at[sp, :, pl.ds(start, part.shape[1])])
        start += part.shape[1]
    in_loads = len(loads)
    load(tokens, tok.at[tp])
    for q in range(nq):
        load(out_pool_w.at[:, pl.ds(q * col_q, col_q)], out_w.at[sp, q, pl.ds(0, pool_ch)])
        load(out_attn_w.at[:, pl.ds(q * col_q, col_q)], out_w.at[sp, q, pl.ds(pool_ch, q_width)])

    def in_sub(owner, u):
        return in_w.at[owner, pl.ds(u * (depth // SUBS), depth // SUBS)]

    out_rows = pool_ch + q_width

    def out_sub(owner, u):
        return out_w.at[owner, u // nr, pl.ds((u % nr) * (out_rows // nr), out_rows // nr)]

    def ring_copy(sub, sems, d, s, u):
        owner = owner_at(place - (s - 1) if d == 0 else place + (s - 1))
        ref = sub(owner, u)
        return pltpu.make_async_remote_copy(
            src_ref=ref,
            dst_ref=ref,
            send_sem=sems[0].at[d, s - 1, u],
            recv_sem=sems[1].at[d, s - 1, u],
            device_id=ahead if d == 0 else behind,
            device_id_type=MESH,
        )

    def ring_arrived(sub, sems, d, s, u):
        owner = owner_at(place - s if d == 0 else place + s)
        ref = sub(owner, u)
        pltpu.make_async_remote_copy(
            src_ref=ref,
            dst_ref=ref,
            send_sem=sems[0].at[d, s - 1, u],
            recv_sem=sems[1].at[d, s - 1, u],
            device_id=behind if d == 0 else ahead,
            device_id_type=MESH,
        ).wait_recv()

    in_ring = (in_sub, (in_send, in_recv))
    ow_ring = (out_sub, (ow_send, ow_recv))

    def ring_start(ring, subs):
        for u in subs:
            for d in range(2):
                ring_copy(*ring, d, 1, u).start()

    def in_half(d, u):
        return u < SUBS // 2 if d == 0 else u >= SUBS // 2

    def ring_step(ring, s, u, last):
        for d in range(2):
            ring_arrived(*ring, d, s, u)
            if not last or in_half(d, u):
                ring_copy(*ring, d, s + 1, u).start()

    def ring_last(ring, k):
        ring_arrived(*ring, 0, half, k)
        ring_arrived(*ring, 1, half, SUBS // 2 + k)

    def ring_sent(ring):
        def full(s, carry):
            for u in range(SUBS):
                for d in range(2):
                    ring_copy(*ring, d, s, u).wait_send()
            return carry

        lax.fori_loop(1, half, full, 0)
        for u in range(SUBS):
            ring_copy(*ring, 0 if in_half(0, u) else 1, half, u).wait_send()

    chunk = rows // CHUNKS

    def tok_rows(slot, j):
        return tok.at[slot, pl.ds(j * chunk, chunk)]

    def over_chips(rel, j, slot):
        return pltpu.make_async_remote_copy(
            src_ref=tok_rows(slot, j),
            dst_ref=tok_rows(slot, j),
            send_sem=tx_send.at[rel - 1, j],
            recv_sem=tx_recv.at[rel - 1, j],
            device_id=chip_peer(rel),
            device_id_type=MESH,
        )

    def over_cores(rel, j, slot):
        return pltpu.make_async_remote_copy(
            src_ref=tok_rows(slot, j),
            dst_ref=tok_rows(slot, j),
            send_sem=td_send.at[rel, j],
            recv_sem=td_recv.at[rel, j],
            device_id=partner,
            device_id_type=MESH,
        )

    pl.semaphore_wait(barrier, len(greeted))
    for copy in loads[:in_loads]:
        copy.wait()
    ring_start(in_ring, range(SUBS))
    loads[in_loads].wait()
    for j in range(CHUNKS):
        for rel in range(1, chips):
            over_chips(rel, j, tp).start()
        over_cores(0, j, tp).start()
    acc[...] = jnp.zeros_like(acc)
    for copy in loads[in_loads + 1 :]:
        copy.wait()

    @pl.when(sp == 0)
    def _():
        kv[pl.ds(0, WINDOW)] = jnp.zeros((WINDOW, kv.shape[1]), kv.dtype)
        pool_pad[pl.ds(0, POOL_PAD)] = jnp.zeros((POOL_PAD, pool_ch), pool_pad.dtype)

    @pl.when(sp == n_sp - 1)
    def _():
        kv[pl.ds(WINDOW + rows, WINDOW)] = jnp.zeros((WINDOW, kv.shape[1]), kv.dtype)
        pool_pad[pl.ds(POOL_PAD + rows, POOL_PAD)] = jnp.zeros((POOL_PAD, pool_ch), pool_pad.dtype)

    def pass_tokens(j):
        for rel in range(1, chips):
            over_chips(rel, j, source_slot(rel)).wait_recv()
            over_cores(rel, j, source_slot(rel)).start()

    norm_rows = 32

    def normalise(j):
        for rel in range(chips):
            slot = source_slot(rel)
            over_cores(rel, j, (slot // 2) * 2 + 1 - core).wait_recv()
            over_cores(rel, j, slot).wait_send()
            if rel:
                over_chips(rel, j, tp).wait_send()

        def tile(i, carry):
            at = pl.ds(pl.multiple_of(j * chunk + i * norm_rows, norm_rows), norm_rows)
            total = jnp.zeros((norm_rows, 1), jnp.float32)
            for slot in range(n_tp):
                floats = tok[slot, at, :].astype(jnp.float32)
                total = total + jnp.sum(floats * floats, axis=-1, keepdims=True)
            scale = lax.rsqrt(total / (feats * n_tp) + epsilon)
            for slot in range(n_tp):
                floats = tok[slot, at, :].astype(jnp.float32)
                tok[slot, at, :] = ((floats * scale) * gain[slot]).astype(jnp.bfloat16)
            return carry

        lax.fori_loop(0, chunk // norm_rows, tile, 0)

    mm_rows = min(rows, 512)

    def block_owner(i):
        return owner_at(place + jnp.where(i % 2 == 1, -((i + 1) // 2), i // 2))

    def project(first, last):
        def step(k, carry):
            i, tile = k // (rows // mm_rows), k % (rows // mm_rows)
            owner = block_owner(i)
            at = pl.ds(pl.multiple_of(tile * mm_rows, mm_rows), mm_rows)
            offset = owner * depth
            part = tok[offset // feats, at, pl.ds(pl.multiple_of(offset % feats, depth), depth)]
            acc[at, :] += jnp.dot(part, in_w[owner], preferred_element_type=jnp.float32)
            return carry

        lax.fori_loop(first * (rows // mm_rows), last * (rows // mm_rows), step, 0)

    ring_step(in_ring, 1, 0, False)
    pass_tokens(0)
    ring_step(in_ring, 1, 1, False)
    normalise(0)
    ring_step(in_ring, 1, 2, False)
    pass_tokens(1)
    ring_step(in_ring, 1, 3, False)
    normalise(1)
    pass_tokens(2)
    ring_step(in_ring, 2, 0, half == 3)
    normalise(2)
    ring_step(in_ring, 2, 1, half == 3)
    pass_tokens(3)
    ring_step(in_ring, 2, 2, half == 3)
    normalise(3)
    project(0, 3)
    ring_step(in_ring, 2, 3, half == 3)
    project(3, 5)

    def middle_in(s, carry):
        for u in range(SUBS):
            ring_step(in_ring, s, u, False)
        project(2 * s - 1, 2 * s + 1)
        return carry

    if half > 4:
        lax.fori_loop(3, half - 1, middle_in, 0)
    if half > 3:
        for u in range(SUBS):
            ring_step(in_ring, half - 1, u, True)
        ring_start(ow_ring, range(SUBS // 2))
        project(n_sp - 3, n_sp - 1)
    for k in range(SUBS // 2):
        ring_last(in_ring, k)
    project(n_sp - 1, n_sp)

    lane = lax.broadcasted_iota(jnp.int32, (GRID_W, LANES), 1)
    take_next = (lane % (HEAD_DIM // 2)) < HEAD_DIM // 4
    kv_cols = 2 * kvw

    def turn(i, carry):
        at = pl.ds(pl.multiple_of(i * GRID_W, GRID_W), GRID_W)
        grid_row = sp * (rows // GRID_W) + i
        cosine = row_cos[pl.ds(grid_row, 1), :] + col_cos[...]
        sine = row_sin[pl.ds(grid_row, 1), :] + col_sin[...]
        to = pl.ds(pl.multiple_of(POOL_PAD + i * GRID_W, POOL_PAD), GRID_W)
        pool_pad[to, :] = acc[at, pl.ds(0, pool_ch)].astype(jnp.bfloat16)

        def turned(start):
            raw = acc[at, pl.ds(start, LANES)]
            other = jnp.where(
                take_next,
                pltpu.roll(raw, LANES - HEAD_DIM // 4, 1),
                pltpu.roll(raw, HEAD_DIM // 4, 1),
            )
            return raw, raw * cosine + other * sine

        for slab in range(q_width // LANES):
            _, values = turned(pool_ch + slab * LANES)
            queries[at, pl.ds(slab * LANES, LANES)] = (values * HEAD_DIM ** (-0.5)).astype(jnp.bfloat16)
        to = pl.ds(pl.multiple_of(WINDOW + i * GRID_W, GRID_W), GRID_W)
        for slab in range(kv_cols // LANES):
            begin = pool_ch + q_width + slab * LANES
            turn_lanes = max(0, min(LANES, kvw - slab * LANES))
            if turn_lanes == 0:
                values = acc[at, pl.ds(begin, LANES)]
            else:
                raw, values = turned(begin)
                if turn_lanes < LANES:
                    values = jnp.where(lane < turn_lanes, values, raw)
            kv[to, pl.ds(slab * LANES, LANES)] = values.astype(jnp.bfloat16)
        return carry

    lax.fori_loop(0, rows // GRID_W, turn, 0)

    def halo(k, up):
        ref, width = ((kv, WINDOW), (pool_pad, POOL_PAD))[k]
        src = pl.ds(rows if up else width, width)
        dst = pl.ds(0 if up else rows + width, width)
        other = ((sp + 1) % n_sp if up else (sp + n_sp - 1) % n_sp, tp)
        return pltpu.make_async_remote_copy(
            src_ref=ref.at[src],
            dst_ref=ref.at[dst],
            send_sem=halo_send.at[k, int(up)],
            recv_sem=halo_recv.at[k, int(up)],
            device_id=other,
            device_id_type=MESH,
        )

    @pl.when(sp < n_sp - 1)
    def _():
        for k in range(2):
            halo(k, True).start()

    @pl.when(sp > 0)
    def _():
        for k in range(2):
            halo(k, False).start()

    ring_start(ow_ring, range(SUBS // 2, SUBS))

    def spread_rows(start, count):
        at = pl.ds(start, count)
        kvx[at, :] = jnp.dot(kv[at, :], spread[...], preferred_element_type=jnp.float32).astype(jnp.bfloat16)

    def spread_tile(i, carry):
        spread_rows(pl.multiple_of((i + 1) * WINDOW, WINDOW), WINDOW)
        return carry

    lax.fori_loop(0, rows // WINDOW, spread_tile, 0)

    span = 3 * WINDOW
    heads_kv = kvw // HEAD_DIM
    group = Q_HEADS // KV_HEADS
    blocks = rows // WINDOW

    def variant(kind, head, upper):
        return pl.ds(((kind * heads_kv + head) * 2 + upper) * LANES, LANES)

    def attend(i, carry):
        at = pl.ds(pl.multiple_of(i * WINDOW, WINDOW), WINDOW)
        keys_at = pl.ds(pl.multiple_of(i * WINDOW, WINDOW), span)
        query = lax.broadcasted_iota(jnp.int32, (WINDOW, span), 0)
        key = lax.broadcasted_iota(jnp.int32, (WINDOW, span), 1)
        low = jnp.where((sp == 0) & (i == 0), WINDOW, 0)
        high = jnp.where((sp == n_sp - 1) & (i == blocks - 1), 2 * WINDOW, span)
        allowed = (key >= jnp.maximum(query, low)) & (key <= jnp.minimum(query + 2 * WINDOW, high - 1))
        for head in range(heads_kv):
            for pair in range(group // 2):
                slab = head * (group // 2) + pair
                q_pair = queries[at, pl.ds(slab * LANES, LANES)]
                result = jnp.zeros((WINDOW, LANES), jnp.float32)
                for upper in range(2):
                    scores = lax.dot_general(
                        q_pair,
                        kvx[keys_at, variant(0, head, upper)],
                        (((1,), (1,)), ((), ())),
                        preferred_element_type=jnp.float32,
                    )
                    scores = jnp.where(allowed, scores, masked_score)
                    logit = sink[slab * 2 + upper]
                    highest = jnp.maximum(jnp.max(scores, axis=-1, keepdims=True), logit)
                    expo = jnp.exp(scores - highest)
                    denominator = jnp.sum(expo, axis=-1, keepdims=True) + jnp.exp(logit - highest)
                    weights = (expo * (1.0 / denominator)).astype(jnp.bfloat16)
                    result += jnp.dot(
                        weights, kvx[keys_at, variant(1, head, upper)], preferred_element_type=jnp.float32
                    )
                mixers[at, pl.ds(pool_ch + slab * LANES, LANES)] = result.astype(jnp.bfloat16)
        return carry

    lax.fori_loop(1, blocks - 1, attend, 0)
    for u in range(2):
        ring_step(ow_ring, 1, u, False)

    @pl.when(sp > 0)
    def _():
        for k in range(2):
            halo(k, True).wait_recv()

    @pl.when(sp < n_sp - 1)
    def _():
        for k in range(2):
            halo(k, False).wait_recv()

    spread_rows(0, WINDOW)
    spread_rows(WINDOW + rows, WINDOW)
    lax.fori_loop(0, 2, lambda e, carry: attend(e * (blocks - 1), carry), 0)
    ring_step(ow_ring, 1, 2, False)

    groups_dev = pool_ch // GROUP_DIM
    tile_rows = 256

    def pool_tile(i, carry):
        at = pl.ds(pl.multiple_of(i * tile_rows, tile_rows), tile_rows)
        wide = tile_rows + 2 * POOL_PAD
        row = lax.broadcasted_iota(jnp.int32, (tile_rows, wide), 0)
        rel = lax.broadcasted_iota(jnp.int32, (tile_rows, wide), 1) - POOL_PAD - row
        position = sp * rows + i * tile_rows + lax.broadcasted_iota(jnp.int32, (tile_rows, LANES), 0)
        for g in range(groups_dev):
            level = (tp * groups_dev + g) % 4
            reach = jnp.where(level == 0, 1, jnp.where(level == 1, 2, jnp.where(level == 2, 4, 8)))
            band = jnp.where((rel >= -reach) & (rel < reach), 1.0, 0.0).astype(jnp.bfloat16)
            cols = pl.ds(g * GROUP_DIM, GROUP_DIM)
            around = pool_pad[pl.ds(pl.multiple_of(i * tile_rows, tile_rows), wide), cols]
            here = pool_pad[pl.ds(pl.multiple_of(i * tile_rows + POOL_PAD, POOL_PAD), tile_rows), cols]
            window_sum = jnp.dot(band, around, preferred_element_type=jnp.float32)
            count = jnp.minimum(position + reach, n_sp * rows) - jnp.maximum(position - reach, 0)
            count = jnp.concatenate([count.astype(jnp.float32)] * (GROUP_DIM // LANES), axis=1)
            pooled = (window_sum / count - here.astype(jnp.float32)).astype(jnp.bfloat16)
            mixed = jnp.dot(pooled, pool_w[g], preferred_element_type=jnp.float32)
            mixers[at, cols] = (mixed * pool_scale[:, cols]).astype(jnp.bfloat16)
        return carry

    lax.fori_loop(0, rows // tile_rows, pool_tile, 0)
    ring_step(ow_ring, 1, 3, False)

    def piece_at(m):
        later = m - nq
        s = later // (2 * nq) + 1
        r = later - (s - 1) * (2 * nq)
        final = s == half
        q = jnp.where(final, r, r // 2)
        delta = jnp.where(final | (r % 2 == 0), -s, s)
        own = m < nq
        return owner_at(place + jnp.where(own, 0, delta)), jnp.where(own, m, q)

    def core_copy(m):
        return pltpu.make_async_remote_copy(
            src_ref=to_core.at[m],
            dst_ref=from_core.at[m],
            send_sem=core_send.at[m],
            recv_sem=core_recv.at[m],
            device_id=partner,
            device_id_type=MESH,
        )

    def chip_copy(m, rel):
        return pltpu.make_async_remote_copy(
            src_ref=own_sum.at[m, (chip + rel) % chips],
            dst_ref=from_chip.at[m, rel - 1],
            send_sem=chip_send.at[m, rel - 1],
            recv_sem=chip_recv.at[m, rel - 1],
            device_id=chip_peer(rel),
            device_id_type=MESH,
        )

    def multiply(m):
        owner, q = piece_at(m)
        for mine, target in ((1 - core, to_core), (core, own_sum)):

            def part(c, carry, mine=mine, target=target):
                at = pl.ds(pl.multiple_of((2 * c + mine) * part_rows, part_rows), part_rows)
                target[m, c] = jnp.dot(
                    mixers[at, :], out_w[owner, q], preferred_element_type=jnp.float32
                ).astype(jnp.bfloat16)
                return carry

            lax.fori_loop(0, chips, part, 0)
            if target is to_core:
                core_copy(m).start()

    def pass_sum(m):
        core_copy(m).wait_recv()
        for rel in range(1, chips):
            c = (chip + rel) % chips
            both = own_sum[m, c].astype(jnp.float32) + from_core[m, c].astype(jnp.float32)
            own_sum[m, c] = both.astype(jnp.bfloat16)
            chip_copy(m, rel).start()

    def total(m):
        owner, q = piece_at(m)
        value = own_sum[m, chip].astype(jnp.float32) + from_core[m, chip].astype(jnp.float32)
        for rel in range(1, chips):
            chip_copy(m, rel).wait_recv()
            value = value + from_chip[m, rel - 1].astype(jnp.float32)
        out[:, pl.ds(pl.multiple_of(owner * cols_dev + q * col_q, col_q), col_q)] = value.astype(out.dtype)

    def piece(m, carry):
        multiply(m)

        @pl.when(m > 0)
        def _():
            pass_sum(m - 1)

        @pl.when(m >= LAG)
        def _():
            total(m - LAG)

        return carry

    lax.fori_loop(0, 3 * nq, piece, 0)

    def out_step(s, last):
        for u in range(SUBS):
            ring_step(ow_ring, s, u, last)
            if (u + 1) % nr == 0:
                first = nq + (s - 1) * 2 * nq + 2 * (u // nr)
                lax.fori_loop(first, first + 2, piece, 0)

    def middle_out(s, carry):
        out_step(s, False)
        return carry

    lax.fori_loop(2, half - 1, middle_out, 0)
    out_step(half - 1, True)
    for k in range(SUBS // 2):
        ring_last(ow_ring, k)
    lax.fori_loop(pieces - nq, pieces, piece, 0)
    pass_sum(pieces - 1)

    def finish(m, carry):
        total(m)
        return carry

    lax.fori_loop(pieces - LAG, pieces, finish, 0)

    ring_sent(in_ring)
    ring_sent(ow_ring)

    @pl.when(sp < n_sp - 1)
    def _():
        for k in range(2):
            halo(k, True).wait_send()

    @pl.when(sp > 0)
    def _():
        for k in range(2):
            halo(k, False).wait_send()

    def sums_sent(m, carry):
        core_copy(m).wait_send()
        for rel in range(1, chips):
            chip_copy(m, rel).wait_send()
        return carry

    lax.fori_loop(0, pieces, sums_sent, 0)


def shards(
    n_sp,
    n_tp,
    tokens,
    norm_gain,
    pool_in_weight,
    query_weight,
    key_weight,
    value_weight,
    pool_weight,
    pool_scale,
    sink_logit,
    out_pool_weight,
    out_attn_weight,
):
    rows, feats = tokens.shape
    depth, pool_ch = pool_in_weight.shape
    q_width = query_weight.shape[1]
    kvw = key_weight.shape[1]
    cols_dev = out_pool_weight.shape[1]
    in_cols = pool_ch + q_width + 2 * kvw
    out_rows = pool_ch + q_width
    half = n_sp // 2
    chips = n_tp // 2
    nq = 2 if cols_dev >= 2 * LANES else 1
    col_q = cols_dev // nq
    pieces = n_sp * nq
    part_rows = rows // n_tp
    if kvw % LANES:
        kv_parts = (jnp.concatenate([key_weight, value_weight], axis=1),)
    else:
        kv_parts = (key_weight, value_weight)
    tables = [jnp.asarray(t) for t in rotary_tables(rows * n_sp)]
    spread = jnp.asarray(spread_matrix(kvw), jnp.bfloat16)
    dims = dict(sp=n_sp, tp=n_tp, kvw=kvw, nq=nq)
    count = len(kv_parts)

    def kernel(*refs):
        layer_kernel(dims, *refs[:3], refs[3 : 3 + count], *refs[3 + count :])

    anywhere = pl.BlockSpec(memory_space=pl.ANY)
    vmem = pl.BlockSpec(memory_space=pltpu.VMEM)
    smem = pl.BlockSpec(memory_space=pltpu.SMEM)
    bf16, f32, dma = jnp.bfloat16, jnp.float32, pltpu.SemaphoreType.DMA
    return pl.pallas_call(
        kernel,
        out_shape=jax.ShapeDtypeStruct((rows // n_tp, cols_dev * n_sp), bf16),
        in_specs=[anywhere] * (5 + count) + [vmem] * 3 + [smem] + [vmem] * 5,
        out_specs=vmem,
        scratch_shapes=[
            pltpu.VMEM((n_tp, rows, feats), bf16),
            pltpu.VMEM((n_sp, depth, in_cols), bf16),
            pltpu.VMEM((n_sp, nq, out_rows, col_q), bf16),
            pltpu.VMEM((rows, in_cols), f32),
            pltpu.VMEM((rows, q_width), bf16),
            pltpu.VMEM((rows + 2 * POOL_PAD, pool_ch), bf16),
            pltpu.VMEM((rows + 2 * WINDOW, 2 * kvw), bf16),
            pltpu.VMEM((rows + 2 * WINDOW, 4 * (kvw // HEAD_DIM) * LANES), bf16),
            pltpu.VMEM((rows, out_rows), bf16),
            pltpu.VMEM((pieces, chips, part_rows, col_q), bf16),
            pltpu.VMEM((pieces, chips, part_rows, col_q), bf16),
            pltpu.VMEM((pieces, chips, part_rows, col_q), bf16),
            pltpu.VMEM((pieces, chips - 1, part_rows, col_q), bf16),
            dma((2 + count + 1 + 2 * nq,)),
            dma((2, half, SUBS)),
            dma((2, half, SUBS)),
            dma((2, half, SUBS)),
            dma((2, half, SUBS)),
            dma((chips - 1, CHUNKS)),
            dma((chips - 1, CHUNKS)),
            dma((chips, CHUNKS)),
            dma((chips, CHUNKS)),
            dma((2, 2)),
            dma((2, 2)),
            dma((pieces,)),
            dma((pieces,)),
            dma((pieces, chips - 1)),
            dma((pieces, chips - 1)),
        ],
        compiler_params=pltpu.CompilerParams(
            collective_id=0, has_side_effects=True, vmem_limit_bytes=67043328
        ),
        name="layer",
    )(
        tokens,
        pool_in_weight,
        query_weight,
        *kv_parts,
        out_pool_weight,
        out_attn_weight,
        norm_gain.reshape(n_tp, 1, feats),
        pool_weight,
        pool_scale.reshape(1, pool_ch),
        sink_logit,
        *tables,
        spread,
    )


def solution(mesh):
    return jax.shard_map(
        functools.partial(shards, mesh.shape["sp"], mesh.shape["tp"]),
        mesh=mesh,
        in_specs=(
            P("sp", "tp"),
            P(),
            P("sp", "tp"),
            P("sp", "tp"),
            P("sp", "tp"),
            P("sp", "tp"),
            P("tp", None, None),
            P("tp"),
            P("tp"),
            P("tp", "sp"),
            P("tp", "sp"),
        ),
        out_specs=P(("sp", "tp"), None),
        check_vma=False,
    )
```

```python
import functools

import jax
import jax.numpy as jnp
import numpy as np
from jax import lax
from jax.experimental import pallas as pl
from jax.experimental.pallas import tpu as pltpu
from jax.sharding import PartitionSpec as P

HEAD_DIM = 64
Q_HEADS = 32
KV_HEADS = 8
GROUP_DIM = 256
WINDOW = 128
GRID_W = 64
LANES = 128
SUBS = 4
CHUNKS = 4
POOL_PAD = 16
LAG = 3

epsilon = 1e-06
rotary_base = 10000.0
masked_score = -1e30
MESH = pl.DeviceIdType.MESH


def rotary_tables(total_rows):
    freq_count = HEAD_DIM // 4
    inverse = np.float32(rotary_base) ** (-np.arange(freq_count, dtype=np.float32) / np.float32(freq_count))
    lane = np.arange(LANES)
    dim = lane % HEAD_DIM
    by_col = (dim // (HEAD_DIM // 2)) == 1
    is_b = (dim % (HEAD_DIM // 2)) // freq_count == 1
    freq = inverse[dim % freq_count]
    sign = np.where(is_b, np.float32(1.0), np.float32(-1.0))
    tables = []
    for count, mine in ((total_rows // GRID_W, ~by_col), (GRID_W, by_col)):
        angle = np.arange(count, dtype=np.float32)[:, None] * freq[None, :]
        tables.append(np.where(mine, np.cos(angle), np.float32(0.0)).astype(np.float32))
        tables.append(np.where(mine, np.sin(angle) * sign, np.float32(0.0)).astype(np.float32))
    return tables


def spread_matrix(kv_width):
    heads = kv_width // HEAD_DIM
    spread = np.zeros((2 * kv_width, 4 * heads * LANES), np.float32)
    for kind in range(2):
        for head in range(heads):
            for half in range(2):
                block = (kind * heads + head) * 2 + half
                for d in range(HEAD_DIM):
                    spread[kind * kv_width + head * HEAD_DIM + d, block * LANES + half * HEAD_DIM + d] = 1.0
    return spread


def layer_kernel(
    dims,
    tokens,
    pool_in_w,
    query_w,
    kv_parts,
    out_pool_w,
    out_attn_w,
    small_refs,
    sink,
    out,
    tok,
    in_w,
    out_w,
    acc,
    queries,
    pool_pad,
    kv,
    kvx,
    mixers,
    to_core,
    own_sum,
    from_core,
    from_chip,
    gain,
    pool_w,
    pool_scale,
    row_cos,
    row_sin,
    col_cos,
    col_sin,
    spread,
    load_sem,
    in_send,
    in_recv,
    ow_send,
    ow_recv,
    tx_send,
    tx_recv,
    td_send,
    td_recv,
    halo_send,
    halo_recv,
    core_send,
    core_recv,
    chip_send,
    chip_recv,
):
    n_sp, n_tp = dims["sp"], dims["tp"]
    rows, feats = tokens.shape
    depth = pool_in_w.shape[0]
    pool_ch = pool_in_w.shape[1]
    q_width = query_w.shape[1]
    kvw = dims["kvw"]
    cols_dev = out_pool_w.shape[1]
    nq = dims["nq"]
    wide = dims["wide"]
    nr = SUBS // nq
    col_q = cols_dev // nq
    half = n_sp // 2
    chips = n_tp // 2
    part_rows = rows // n_tp
    pieces = n_sp * nq

    sp = lax.axis_index("sp")
    tp = lax.axis_index("tp")
    chip = tp // 2
    core = tp % 2
    place = jnp.where(sp % 2 == 0, sp // 2, n_sp - 1 - sp // 2)

    def owner_at(spot):
        spot = (spot + n_sp) % n_sp
        return jnp.where(spot < half, 2 * spot, 2 * (n_sp - 1 - spot) + 1)

    ahead = (owner_at(place + 1), tp)
    behind = (owner_at(place - 1), tp)
    partner = (sp, chip * 2 + 1 - core)

    def chip_peer(rel):
        return (sp, ((chip + rel) % chips) * 2 + core)

    def source_slot(rel):
        return ((chip - rel + chips) % chips) * 2 + core

    barrier = pltpu.get_barrier_semaphore()
    greeted = [ahead, behind, ((sp + 1) % n_sp, tp), ((sp + n_sp - 1) % n_sp, tp), partner]
    greeted += [chip_peer(rel) for rel in range(1, chips)]
    for other in greeted:
        pl.semaphore_signal(barrier, inc=1, device_id=other, device_id_type=MESH)

    loads = []

    def load(src, dst):
        copy = pltpu.make_async_copy(src, dst, load_sem.at[len(loads)])
        copy.start()
        loads.append(copy)

    sub_rows = depth // SUBS
    for u in range(SUBS):
        at = pl.ds(u * sub_rows, sub_rows)
        start = 0
        for part in (pool_in_w, query_w, *kv_parts):
            load(part.at[at], in_w.at[sp, at, pl.ds(start, part.shape[1])])
            start += part.shape[1]
    in_loads = len(loads) // SUBS
    load(tokens, tok.at[tp])
    quarters = SUBS if wide else 1
    col_w = cols_dev // quarters
    for q in range(quarters):
        load(out_pool_w.at[:, pl.ds(q * col_w, col_w)], out_w.at[sp, q, pl.ds(0, pool_ch)])
        load(out_attn_w.at[:, pl.ds(q * col_w, col_w)], out_w.at[sp, q, pl.ds(pool_ch, q_width)])
    for src, dst in zip(small_refs, (gain, pool_w, pool_scale, row_cos, row_sin, col_cos, col_sin, spread)):
        load(src, dst)

    def in_sub(owner, u):
        return in_w.at[owner, pl.ds(u * (depth // SUBS), depth // SUBS)]

    out_rows = pool_ch + q_width

    def out_sub(owner, u):
        if wide:
            return out_w.at[owner, u]
        return out_w.at[owner, 0, pl.ds(u * (out_rows // SUBS), out_rows // SUBS)]

    def ring_copy(sub, sems, d, s, u):
        owner = owner_at(place - (s - 1) if d == 0 else place + (s - 1))
        ref = sub(owner, u)
        return pltpu.make_async_remote_copy(
            src_ref=ref,
            dst_ref=ref,
            send_sem=sems[0].at[d, s - 1, u],
            recv_sem=sems[1].at[d, s - 1, u],
            device_id=ahead if d == 0 else behind,
            device_id_type=MESH,
        )

    def ring_arrived(sub, sems, d, s, u):
        owner = owner_at(place - s if d == 0 else place + s)
        ref = sub(owner, u)
        pltpu.make_async_remote_copy(
            src_ref=ref,
            dst_ref=ref,
            send_sem=sems[0].at[d, s - 1, u],
            recv_sem=sems[1].at[d, s - 1, u],
            device_id=behind if d == 0 else ahead,
            device_id_type=MESH,
        ).wait_recv()

    in_ring = (in_sub, (in_send, in_recv))
    ow_ring = (out_sub, (ow_send, ow_recv))

    def ring_start(ring, subs):
        for u in subs:
            for d in range(2):
                ring_copy(*ring, d, 1, u).start()

    def in_half(d, u):
        return u < SUBS // 2 if d == 0 else u >= SUBS // 2

    def ring_step(ring, s, u, last):
        for d in range(2):
            ring_arrived(*ring, d, s, u)
            if not last or in_half(d, u):
                ring_copy(*ring, d, s + 1, u).start()

    def ring_last(ring, k):
        ring_arrived(*ring, 0, half, k)
        ring_arrived(*ring, 1, half, SUBS // 2 + k)

    def ring_sent(ring):
        def full(s, carry):
            for u in range(SUBS):
                for d in range(2):
                    ring_copy(*ring, d, s, u).wait_send()
            return carry

        lax.fori_loop(1, half, full, 0)
        for u in range(SUBS):
            ring_copy(*ring, 0 if in_half(0, u) else 1, half, u).wait_send()

    chunk = rows // CHUNKS

    def tok_rows(slot, j):
        return tok.at[slot, pl.ds(j * chunk, chunk)]

    def over_chips(rel, j, slot):
        return pltpu.make_async_remote_copy(
            src_ref=tok_rows(slot, j),
            dst_ref=tok_rows(slot, j),
            send_sem=tx_send.at[rel - 1, j],
            recv_sem=tx_recv.at[rel - 1, j],
            device_id=chip_peer(rel),
            device_id_type=MESH,
        )

    def over_cores(rel, j, slot):
        return pltpu.make_async_remote_copy(
            src_ref=tok_rows(slot, j),
            dst_ref=tok_rows(slot, j),
            send_sem=td_send.at[rel, j],
            recv_sem=td_recv.at[rel, j],
            device_id=partner,
            device_id_type=MESH,
        )

    pl.semaphore_wait(barrier, len(greeted))
    for u in range(SUBS):
        for copy in loads[u * in_loads : (u + 1) * in_loads]:
            copy.wait()
        ring_start(in_ring, (u,))
    loads[SUBS * in_loads].wait()
    for j in range(CHUNKS):
        for rel in range(1, chips):
            over_chips(rel, j, tp).start()
        over_cores(0, j, tp).start()
    acc[...] = jnp.zeros_like(acc)
    for copy in loads[SUBS * in_loads + 1 :]:
        copy.wait()

    @pl.when(sp == 0)
    def _():
        kv[pl.ds(0, WINDOW)] = jnp.zeros((WINDOW, kv.shape[1]), kv.dtype)
        pool_pad[pl.ds(0, POOL_PAD)] = jnp.zeros((POOL_PAD, pool_ch), pool_pad.dtype)

    @pl.when(sp == n_sp - 1)
    def _():
        kv[pl.ds(WINDOW + rows, WINDOW)] = jnp.zeros((WINDOW, kv.shape[1]), kv.dtype)
        pool_pad[pl.ds(POOL_PAD + rows, POOL_PAD)] = jnp.zeros((POOL_PAD, pool_ch), pool_pad.dtype)

    def pass_tokens(j):
        for rel in range(1, chips):
            over_chips(rel, j, source_slot(rel)).wait_recv()
            over_cores(rel, j, source_slot(rel)).start()

    norm_rows = 32

    def normalise(j):
        for rel in range(chips):
            slot = source_slot(rel)
            over_cores(rel, j, (slot // 2) * 2 + 1 - core).wait_recv()
            over_cores(rel, j, slot).wait_send()
            if rel:
                over_chips(rel, j, tp).wait_send()

        def tile(i, carry):
            at = pl.ds(pl.multiple_of(j * chunk + i * norm_rows, norm_rows), norm_rows)
            total = jnp.zeros((norm_rows, 1), jnp.float32)
            for slot in range(n_tp):
                floats = tok[slot, at, :].astype(jnp.float32)
                total = total + jnp.sum(floats * floats, axis=-1, keepdims=True)
            scale = lax.rsqrt(total / (feats * n_tp) + epsilon)
            for slot in range(n_tp):
                floats = tok[slot, at, :].astype(jnp.float32)
                tok[slot, at, :] = ((floats * scale) * gain[slot]).astype(jnp.bfloat16)
            return carry

        lax.fori_loop(0, chunk // norm_rows, tile, 0)

    mm_rows = min(rows, 512)

    def block_owner(i):
        return owner_at(place + jnp.where(i % 2 == 1, -((i + 1) // 2), i // 2))

    def project(first, last):
        def step(k, carry):
            i, tile = k // (rows // mm_rows), k % (rows // mm_rows)
            owner = block_owner(i)
            at = pl.ds(pl.multiple_of(tile * mm_rows, mm_rows), mm_rows)
            offset = owner * depth
            part = tok[offset // feats, at, pl.ds(pl.multiple_of(offset % feats, depth), depth)]
            acc[at, :] += jnp.dot(part, in_w[owner], preferred_element_type=jnp.float32)
            return carry

        lax.fori_loop(first * (rows // mm_rows), last * (rows // mm_rows), step, 0)

    ring_step(in_ring, 1, 0, False)
    pass_tokens(0)
    ring_step(in_ring, 1, 1, False)
    normalise(0)
    ring_step(in_ring, 1, 2, False)
    pass_tokens(1)
    ring_step(in_ring, 1, 3, False)
    normalise(1)
    pass_tokens(2)
    ring_step(in_ring, 2, 0, half == 3)
    normalise(2)
    ring_step(in_ring, 2, 1, half == 3)
    pass_tokens(3)
    ring_step(in_ring, 2, 2, half == 3)
    normalise(3)
    project(0, 3)
    ring_step(in_ring, 2, 3, half == 3)
    project(3, 5)

    def middle_in(s, carry):
        for u in range(SUBS):
            ring_step(in_ring, s, u, False)
        project(2 * s - 1, 2 * s + 1)
        return carry

    if half > 4:
        lax.fori_loop(3, half - 1, middle_in, 0)
    if half > 3:
        for u in range(SUBS):
            ring_step(in_ring, half - 1, u, True)
        ring_start(ow_ring, range(SUBS // 2))
        project(n_sp - 3, n_sp - 1)
    for k in range(SUBS // 2):
        ring_last(in_ring, k)
    project(n_sp - 1, n_sp)

    lane = lax.broadcasted_iota(jnp.int32, (GRID_W, LANES), 1)
    take_next = (lane % (HEAD_DIM // 2)) < HEAD_DIM // 4
    kv_cols = 2 * kvw

    def turn(i, carry):
        at = pl.ds(pl.multiple_of(i * GRID_W, GRID_W), GRID_W)
        grid_row = sp * (rows // GRID_W) + i
        cosine = row_cos[pl.ds(grid_row, 1), :] + col_cos[...]
        sine = row_sin[pl.ds(grid_row, 1), :] + col_sin[...]
        to = pl.ds(pl.multiple_of(POOL_PAD + i * GRID_W, POOL_PAD), GRID_W)
        pool_pad[to, :] = acc[at, pl.ds(0, pool_ch)].astype(jnp.bfloat16)

        def turned(start):
            raw = acc[at, pl.ds(start, LANES)]
            other = jnp.where(
                take_next,
                pltpu.roll(raw, LANES - HEAD_DIM // 4, 1),
                pltpu.roll(raw, HEAD_DIM // 4, 1),
            )
            return raw, raw * cosine + other * sine

        for slab in range(q_width // LANES):
            _, values = turned(pool_ch + slab * LANES)
            queries[at, pl.ds(slab * LANES, LANES)] = (values * HEAD_DIM ** (-0.5)).astype(jnp.bfloat16)
        to = pl.ds(pl.multiple_of(WINDOW + i * GRID_W, GRID_W), GRID_W)
        for slab in range(kv_cols // LANES):
            begin = pool_ch + q_width + slab * LANES
            turn_lanes = max(0, min(LANES, kvw - slab * LANES))
            if turn_lanes == 0:
                values = acc[at, pl.ds(begin, LANES)]
            else:
                raw, values = turned(begin)
                if turn_lanes < LANES:
                    values = jnp.where(lane < turn_lanes, values, raw)
            kv[to, pl.ds(slab * LANES, LANES)] = values.astype(jnp.bfloat16)
        return carry

    lax.fori_loop(0, rows // GRID_W, turn, 0)

    def halo(k, up):
        ref, width = ((kv, WINDOW), (pool_pad, POOL_PAD))[k]
        src = pl.ds(rows if up else width, width)
        dst = pl.ds(0 if up else rows + width, width)
        other = ((sp + 1) % n_sp if up else (sp + n_sp - 1) % n_sp, tp)
        return pltpu.make_async_remote_copy(
            src_ref=ref.at[src],
            dst_ref=ref.at[dst],
            send_sem=halo_send.at[k, int(up)],
            recv_sem=halo_recv.at[k, int(up)],
            device_id=other,
            device_id_type=MESH,
        )

    @pl.when(sp < n_sp - 1)
    def _():
        for k in range(2):
            halo(k, True).start()

    @pl.when(sp > 0)
    def _():
        for k in range(2):
            halo(k, False).start()

    ring_start(ow_ring, range(SUBS // 2, SUBS))

    def spread_rows(start, count):
        at = pl.ds(start, count)
        kvx[at, :] = jnp.dot(kv[at, :], spread[...], preferred_element_type=jnp.float32).astype(jnp.bfloat16)

    def spread_tile(i, carry):
        spread_rows(pl.multiple_of((i + 1) * WINDOW, WINDOW), WINDOW)
        return carry

    lax.fori_loop(0, rows // WINDOW, spread_tile, 0)

    span = 3 * WINDOW
    heads_kv = kvw // HEAD_DIM
    group = Q_HEADS // KV_HEADS
    blocks = rows // WINDOW

    def variant(kind, head, upper):
        return pl.ds(((kind * heads_kv + head) * 2 + upper) * LANES, LANES)

    def attend(i, carry):
        at = pl.ds(pl.multiple_of(i * WINDOW, WINDOW), WINDOW)
        keys_at = pl.ds(pl.multiple_of(i * WINDOW, WINDOW), span)
        query = lax.broadcasted_iota(jnp.int32, (WINDOW, span), 0)
        key = lax.broadcasted_iota(jnp.int32, (WINDOW, span), 1)
        low = jnp.where((sp == 0) & (i == 0), WINDOW, 0)
        high = jnp.where((sp == n_sp - 1) & (i == blocks - 1), 2 * WINDOW, span)
        allowed = (key >= jnp.maximum(query, low)) & (key <= jnp.minimum(query + 2 * WINDOW, high - 1))
        for head in range(heads_kv):
            for pair in range(group // 2):
                slab = head * (group // 2) + pair
                q_pair = queries[at, pl.ds(slab * LANES, LANES)]
                result = jnp.zeros((WINDOW, LANES), jnp.float32)
                for upper in range(2):
                    scores = lax.dot_general(
                        q_pair,
                        kvx[keys_at, variant(0, head, upper)],
                        (((1,), (1,)), ((), ())),
                        preferred_element_type=jnp.float32,
                    )
                    scores = jnp.where(allowed, scores, masked_score)
                    logit = sink[slab * 2 + upper]
                    highest = jnp.maximum(jnp.max(scores, axis=-1, keepdims=True), logit)
                    expo = jnp.exp(scores - highest)
                    denominator = jnp.sum(expo, axis=-1, keepdims=True) + jnp.exp(logit - highest)
                    weights = (expo * (1.0 / denominator)).astype(jnp.bfloat16)
                    result += jnp.dot(
                        weights, kvx[keys_at, variant(1, head, upper)], preferred_element_type=jnp.float32
                    )
                mixers[at, pl.ds(pool_ch + slab * LANES, LANES)] = result.astype(jnp.bfloat16)
        return carry

    lax.fori_loop(1, blocks - 1, attend, 0)
    for u in range(2):
        ring_step(ow_ring, 1, u, False)

    @pl.when(sp > 0)
    def _():
        for k in range(2):
            halo(k, True).wait_recv()

    @pl.when(sp < n_sp - 1)
    def _():
        for k in range(2):
            halo(k, False).wait_recv()

    spread_rows(0, WINDOW)
    spread_rows(WINDOW + rows, WINDOW)
    lax.fori_loop(0, 2, lambda e, carry: attend(e * (blocks - 1), carry), 0)
    ring_step(ow_ring, 1, 2, False)

    groups_dev = pool_ch // GROUP_DIM
    tile_rows = 256

    def pool_tile(i, carry):
        at = pl.ds(pl.multiple_of(i * tile_rows, tile_rows), tile_rows)
        wide = tile_rows + 2 * POOL_PAD
        row = lax.broadcasted_iota(jnp.int32, (tile_rows, wide), 0)
        rel = lax.broadcasted_iota(jnp.int32, (tile_rows, wide), 1) - POOL_PAD - row
        position = sp * rows + i * tile_rows + lax.broadcasted_iota(jnp.int32, (tile_rows, LANES), 0)
        for g in range(groups_dev):
            level = (tp * groups_dev + g) % 4
            reach = jnp.where(level == 0, 1, jnp.where(level == 1, 2, jnp.where(level == 2, 4, 8)))
            band = jnp.where((rel >= -reach) & (rel < reach), 1.0, 0.0).astype(jnp.bfloat16)
            cols = pl.ds(g * GROUP_DIM, GROUP_DIM)
            around = pool_pad[pl.ds(pl.multiple_of(i * tile_rows, tile_rows), wide), cols]
            here = pool_pad[pl.ds(pl.multiple_of(i * tile_rows + POOL_PAD, POOL_PAD), tile_rows), cols]
            window_sum = jnp.dot(band, around, preferred_element_type=jnp.float32)
            count = jnp.minimum(position + reach, n_sp * rows) - jnp.maximum(position - reach, 0)
            count = jnp.concatenate([count.astype(jnp.float32)] * (GROUP_DIM // LANES), axis=1)
            pooled = (window_sum / count - here.astype(jnp.float32)).astype(jnp.bfloat16)
            mixed = jnp.dot(pooled, pool_w[g], preferred_element_type=jnp.float32)
            mixers[at, cols] = (mixed * pool_scale[:, cols]).astype(jnp.bfloat16)
        return carry

    lax.fori_loop(0, rows // tile_rows, pool_tile, 0)
    ring_step(ow_ring, 1, 3, False)

    def piece_at(m):
        later = m - nq
        s = later // (2 * nq) + 1
        r = later - (s - 1) * (2 * nq)
        final = s == half
        q = jnp.where(final, r, r // 2)
        delta = jnp.where(final | (r % 2 == 0), -s, s)
        own = m < nq
        return owner_at(place + jnp.where(own, 0, delta)), jnp.where(own, m, q)

    def weight_quarters(m, q):
        final = m >= pieces - nq
        return jnp.where(final, q, 2 * q), jnp.where(final, q + SUBS // 2, 2 * q + 1)

    def core_copy(m, rel):
        c = (chip + rel) % chips
        return pltpu.make_async_remote_copy(
            src_ref=to_core.at[m, c],
            dst_ref=from_core.at[m, c],
            send_sem=core_send.at[m, rel],
            recv_sem=core_recv.at[m, rel],
            device_id=partner,
            device_id_type=MESH,
        )

    def chip_copy(m, rel):
        return pltpu.make_async_remote_copy(
            src_ref=own_sum.at[m, (chip + rel) % chips],
            dst_ref=from_chip.at[m, rel - 1],
            send_sem=chip_send.at[m, rel - 1],
            recv_sem=chip_recv.at[m, rel - 1],
            device_id=chip_peer(rel),
            device_id_type=MESH,
        )

    def multiply(m):
        owner, q = piece_at(m)

        def part(k, carry):
            rel = (k // 2 + 1) % chips
            c = (chip + rel) % chips
            mine = jnp.where(k % 2 == 0, 1 - core, core)
            at = pl.ds(pl.multiple_of((2 * c + mine) * part_rows, part_rows), part_rows)
            if wide:
                first, second = weight_quarters(m, q)
                weight = jnp.concatenate([out_w[owner, first], out_w[owner, second]], axis=1)
            else:
                weight = out_w[owner, q]
            result = jnp.dot(mixers[at, :], weight, preferred_element_type=jnp.float32).astype(jnp.bfloat16)

            @pl.when(k % 2 == 0)
            def _():
                to_core[m, c] = result
                core_copy(m, rel).start()

            @pl.when(k % 2 == 1)
            def _():
                own_sum[m, c] = result

            return carry

        lax.fori_loop(0, n_tp, part, 0)

    def pass_sum(m):
        for rel in range(1, chips):
            core_copy(m, rel).wait_recv()
            c = (chip + rel) % chips
            both = own_sum[m, c].astype(jnp.float32) + from_core[m, c].astype(jnp.float32)
            own_sum[m, c] = both.astype(jnp.bfloat16)
            chip_copy(m, rel).start()

    def total(m):
        owner, q = piece_at(m)
        core_copy(m, 0).wait_recv()
        value = own_sum[m, chip].astype(jnp.float32) + from_core[m, chip].astype(jnp.float32)
        for rel in range(1, chips):
            chip_copy(m, rel).wait_recv()
            value = value + from_chip[m, rel - 1].astype(jnp.float32)
        value = value.astype(out.dtype)
        if wide:
            for k, quarter in enumerate(weight_quarters(m, q)):
                to = pl.ds(pl.multiple_of(owner * cols_dev + quarter * col_w, col_w), col_w)
                out[:, to] = value[:, k * col_w : (k + 1) * col_w]
        else:
            out[:, pl.ds(pl.multiple_of(owner * cols_dev, cols_dev), cols_dev)] = value

    def piece(m, carry):
        multiply(m)
        pass_sum(m)

        @pl.when(m >= LAG)
        def _():
            total(m - LAG)

        return carry

    lax.fori_loop(0, 3 * nq, piece, 0)

    def out_step(s, last):
        for u in range(SUBS):
            ring_step(ow_ring, s, u, last)
            if (u + 1) % nr == 0:
                first = nq + (s - 1) * 2 * nq + 2 * (u // nr)
                lax.fori_loop(first, first + 2, piece, 0)

    def middle_out(s, carry):
        out_step(s, False)
        return carry

    lax.fori_loop(2, half - 1, middle_out, 0)
    out_step(half - 1, True)
    for k in range(SUBS // 2):
        ring_last(ow_ring, k)
        if wide:
            lax.fori_loop(pieces - nq + k, pieces - nq + k + 1, piece, 0)
    if not wide:
        lax.fori_loop(pieces - nq, pieces, piece, 0)

    def finish(m, carry):
        total(m)
        return carry

    lax.fori_loop(pieces - LAG, pieces, finish, 0)

    ring_sent(in_ring)
    ring_sent(ow_ring)

    @pl.when(sp < n_sp - 1)
    def _():
        for k in range(2):
            halo(k, True).wait_send()

    @pl.when(sp > 0)
    def _():
        for k in range(2):
            halo(k, False).wait_send()

    def sums_sent(m, carry):
        core_copy(m, 0).wait_send()
        for rel in range(1, chips):
            core_copy(m, rel).wait_send()
            chip_copy(m, rel).wait_send()
        return carry

    lax.fori_loop(0, pieces, sums_sent, 0)


def shards(
    n_sp,
    n_tp,
    tokens,
    norm_gain,
    pool_in_weight,
    query_weight,
    key_weight,
    value_weight,
    pool_weight,
    pool_scale,
    sink_logit,
    out_pool_weight,
    out_attn_weight,
):
    rows, feats = tokens.shape
    depth, pool_ch = pool_in_weight.shape
    q_width = query_weight.shape[1]
    kvw = key_weight.shape[1]
    cols_dev = out_pool_weight.shape[1]
    in_cols = pool_ch + q_width + 2 * kvw
    out_rows = pool_ch + q_width
    half = n_sp // 2
    chips = n_tp // 2
    wide = cols_dev == SUBS * LANES
    nq = SUBS // 2 if wide else 1
    col_q = cols_dev // nq
    pieces = n_sp * nq
    part_rows = rows // n_tp
    if kvw % LANES:
        kv_parts = (jnp.concatenate([key_weight, value_weight], axis=1),)
    else:
        kv_parts = (key_weight, value_weight)
    tables = [jnp.asarray(t) for t in rotary_tables(rows * n_sp)]
    spread = jnp.asarray(spread_matrix(kvw), jnp.bfloat16)
    dims = dict(sp=n_sp, tp=n_tp, kvw=kvw, nq=nq, wide=wide)
    small = (norm_gain.reshape(n_tp, 1, feats), pool_weight, pool_scale.reshape(1, pool_ch), *tables, spread)
    count = len(kv_parts)

    def kernel(*refs):
        a, b = 3 + count, 5 + count
        layer_kernel(dims, *refs[:3], refs[3:a], *refs[a:b], refs[b : b + len(small)], *refs[b + len(small) :])

    anywhere = pl.BlockSpec(memory_space=pl.ANY)
    vmem = pl.BlockSpec(memory_space=pltpu.VMEM)
    smem = pl.BlockSpec(memory_space=pltpu.SMEM)
    bf16, f32, dma = jnp.bfloat16, jnp.float32, pltpu.SemaphoreType.DMA
    return pl.pallas_call(
        kernel,
        out_shape=pltpu.VMEM((rows // n_tp, cols_dev * n_sp), bf16),
        in_specs=[anywhere] * (5 + count + len(small)) + [smem],
        out_specs=vmem,
        scratch_shapes=[
            pltpu.VMEM((n_tp, rows, feats), bf16),
            pltpu.VMEM((n_sp, depth, in_cols), bf16),
            pltpu.VMEM((n_sp, SUBS if wide else 1, out_rows, LANES if wide else cols_dev), bf16),
            pltpu.VMEM((rows, in_cols), f32),
            pltpu.VMEM((rows, q_width), bf16),
            pltpu.VMEM((rows + 2 * POOL_PAD, pool_ch), bf16),
            pltpu.VMEM((rows + 2 * WINDOW, 2 * kvw), bf16),
            pltpu.VMEM((rows + 2 * WINDOW, 4 * (kvw // HEAD_DIM) * LANES), bf16),
            pltpu.VMEM((rows, out_rows), bf16),
            pltpu.VMEM((pieces, chips, part_rows, col_q), bf16),
            pltpu.VMEM((pieces, chips, part_rows, col_q), bf16),
            pltpu.VMEM((pieces, chips, part_rows, col_q), bf16),
            pltpu.VMEM((pieces, chips - 1, part_rows, col_q), bf16),
            *[pltpu.VMEM(value.shape, value.dtype) for value in small],
            dma((SUBS * (2 + count) + 1 + 2 * (SUBS if wide else 1) + len(small),)),
            dma((2, half, SUBS)),
            dma((2, half, SUBS)),
            dma((2, half, SUBS)),
            dma((2, half, SUBS)),
            dma((chips - 1, CHUNKS)),
            dma((chips - 1, CHUNKS)),
            dma((chips, CHUNKS)),
            dma((chips, CHUNKS)),
            dma((2, 2)),
            dma((2, 2)),
            dma((pieces, chips)),
            dma((pieces, chips)),
            dma((pieces, chips - 1)),
            dma((pieces, chips - 1)),
        ],
        compiler_params=pltpu.CompilerParams(
            collective_id=0, has_side_effects=True, vmem_limit_bytes=61 * 2**20
        ),
        name="layer",
    )(
        tokens,
        pool_in_weight,
        query_weight,
        *kv_parts,
        out_pool_weight,
        out_attn_weight,
        *small,
        sink_logit,
    )


def solution(mesh):
    return jax.shard_map(
        functools.partial(shards, mesh.shape["sp"], mesh.shape["tp"]),
        mesh=mesh,
        in_specs=(
            P("sp", "tp"),
            P(),
            P("sp", "tp"),
            P("sp", "tp"),
            P("sp", "tp"),
            P("sp", "tp"),
            P("tp", None, None),
            P("tp"),
            P("tp"),
            P("tp", "sp"),
            P("tp", "sp"),
        ),
        out_specs=P(("sp", "tp"), None),
        check_vma=False,
    )
```

```python
import functools

import jax
import jax.numpy as jnp
import numpy as np
from jax import lax
from jax.experimental import pallas as pl
from jax.experimental.pallas import tpu as pltpu
from jax.sharding import PartitionSpec as P

HEAD_DIM = 64
Q_HEADS = 32
KV_HEADS = 8
GROUP_DIM = 256
WINDOW = 128
GRID_W = 64
LANES = 128
SUBS = 4
CHUNKS = 4
POOL_PAD = 16
LAG = 3

epsilon = 1e-06
rotary_base = 10000.0
masked_score = -1e30
MESH = pl.DeviceIdType.MESH


def rotary_tables(total_rows):
    freq_count = HEAD_DIM // 4
    inverse = np.float32(rotary_base) ** (-np.arange(freq_count, dtype=np.float32) / np.float32(freq_count))
    lane = np.arange(LANES)
    dim = lane % HEAD_DIM
    by_col = (dim // (HEAD_DIM // 2)) == 1
    is_b = (dim % (HEAD_DIM // 2)) // freq_count == 1
    freq = inverse[dim % freq_count]
    sign = np.where(is_b, np.float32(1.0), np.float32(-1.0))
    tables = []
    for count, mine in ((total_rows // GRID_W, ~by_col), (GRID_W, by_col)):
        angle = np.arange(count, dtype=np.float32)[:, None] * freq[None, :]
        tables.append(np.where(mine, np.cos(angle), np.float32(0.0)).astype(np.float32))
        tables.append(np.where(mine, np.sin(angle) * sign, np.float32(0.0)).astype(np.float32))
    return tables


def spread_matrix(heads, width):
    spread = np.zeros((width, 2 * heads * LANES), np.float32)
    for head in range(heads):
        for half in range(2):
            for d in range(HEAD_DIM):
                spread[head * HEAD_DIM + d, (head * 2 + half) * LANES + half * HEAD_DIM + d] = 1.0
    return spread


def layer_kernel(
    dims,
    tokens,
    pool_in_w,
    query_w,
    key_w,
    value_w,
    out_pool_w,
    out_attn_w,
    small_refs,
    sink,
    out,
    tok,
    in_a,
    in_b,
    mate_a,
    mate_b,
    out_w,
    acc,
    queries,
    pool_pad,
    kv,
    stage_pool,
    stage_q,
    stage_kv,
    kvx,
    mixers,
    to_core,
    own_sum,
    from_core,
    from_chip,
    gain,
    pool_w,
    pool_scale,
    row_cos,
    row_sin,
    col_cos,
    col_sin,
    spread,
    load_sem,
    pw_send,
    pw_recv,
    in_send,
    in_recv,
    ow_send,
    ow_recv,
    tx_send,
    tx_recv,
    td_send,
    td_recv,
    ty_send,
    ty_recv,
    swap_send,
    swap_recv,
    halo_send,
    halo_recv,
    core_send,
    core_recv,
    chip_send,
    chip_recv,
):
    n_sp, n_tp = dims["sp"], dims["tp"]
    rows, feats = tokens.shape
    depth = pool_in_w.shape[0]
    pool_ch = pool_in_w.shape[1]
    q_width = query_w.shape[1]
    heads_kv = dims["heads_kv"]
    kv_width = key_w.shape[1]
    pool_half = pool_ch // 2
    q_half = q_width // 2
    cols_dev = out_pool_w.shape[1]
    nq = dims["nq"]
    wide = dims["wide"]
    nr = SUBS // nq
    col_q = cols_dev // nq
    half = n_sp // 2
    chips = n_tp // 2
    part_rows = rows // n_tp
    pieces = n_sp * nq

    sp = lax.axis_index("sp")
    tp = lax.axis_index("tp")
    chip = tp // 2
    core = tp % 2
    place = jnp.where(sp % 2 == 0, sp // 2, n_sp - 1 - sp // 2)
    pairs = n_sp // 2
    pair = sp // 2
    member = sp % 2
    mate = (pair * 2 + 1 - member, tp)

    def pair_at(offset, which):
        return (((pair + offset + pairs) % pairs) * 2 + which, tp)

    def owner_at(spot):
        spot = (spot + n_sp) % n_sp
        return jnp.where(spot < half, 2 * spot, 2 * (n_sp - 1 - spot) + 1)

    ahead = (owner_at(place + 1), tp)
    behind = (owner_at(place - 1), tp)
    partner = (sp, chip * 2 + 1 - core)

    def chip_peer(rel):
        return (sp, ((chip + rel) % chips) * 2 + core)

    def source_slot(rel):
        return ((chip - rel + chips) % chips) * 2 + core

    barrier = pltpu.get_barrier_semaphore()
    greeted = [ahead, behind, mate, partner]
    greeted += [pair_at(offset, which) for offset in (1, -1) for which in (member, 1 - member)]
    greeted += [chip_peer(rel) for rel in range(1, chips)]
    for other in greeted:
        pl.semaphore_signal(barrier, inc=1, device_id=other, device_id_type=MESH)

    loads = []

    def load(src, dst):
        copy = pltpu.make_async_copy(src, dst, load_sem.at[6 + len(loads)])
        copy.start()
        loads.append(copy)

    in_w = (in_a, in_b)

    def local_loads(which, heads_to, pool_to, first):
        parts = (
            (query_w.at[:, pl.ds(which * q_half, q_half)], heads_to.at[:, pl.ds(0, q_half)]),
            (key_w if which == 0 else value_w, heads_to.at[:, pl.ds(q_half, kv_width)]),
            (pool_in_w.at[:, pl.ds(which * pool_half, pool_half)], pool_to),
        )
        return [pltpu.make_async_copy(src, dst, load_sem.at[first + k]) for k, (src, dst) in enumerate(parts)]

    def own_load(which):
        return local_loads(which, in_a.at[sp], in_b.at[sp], 0)

    def mate_load(which):
        return local_loads(which, mate_a, mate_b, 3)

    def mate_weights(p):
        return pltpu.make_async_remote_copy(
            src_ref=(mate_a, mate_b)[p],
            dst_ref=in_w[p].at[sp],
            send_sem=pw_send.at[p],
            recv_sem=pw_recv.at[p],
            device_id=mate,
            device_id_type=MESH,
        )

    for which in range(2):

        @pl.when(member == which)
        def _(which=which):
            for copy in own_load(which) + mate_load(1 - which):
                copy.start()

    load(tokens, tok.at[member, tp])
    quarters = SUBS if wide else 1
    col_w = cols_dev // quarters
    for q in range(quarters):
        load(out_pool_w.at[:, pl.ds(q * col_w, col_w)], out_w.at[sp, q, pl.ds(0, pool_ch)])
        load(out_attn_w.at[:, pl.ds(q * col_w, col_w)], out_w.at[sp, q, pl.ds(pool_ch, q_width)])
    for src, dst in zip(small_refs, (gain, pool_w, pool_scale, row_cos, row_sin, col_cos, col_sin, spread)):
        load(src, dst)

    pass_cols = (pl.ds(pool_half, q_half + kv_width), pl.ds(0, pool_half))

    def in_sub(p, which_pair, u):
        owner = which_pair * 2 + (member if u == 0 else 1 - member)
        return in_w[p].at[owner]

    def line_exists(d, s):
        return pair >= s if d == 0 else pair < pairs - s

    def line_ref_copy(p, d, s, u, ref, target):
        return pltpu.make_async_remote_copy(
            src_ref=ref,
            dst_ref=ref,
            send_sem=in_send.at[p, d, s - 1, u],
            recv_sem=in_recv.at[p, d, s - 1, u],
            device_id=target,
            device_id_type=MESH,
        )

    def line_copy(p, d, s, u):
        ref = in_sub(p, pair - (s - 1) if d == 0 else pair + (s - 1), u)
        return line_ref_copy(p, d, s, u, ref, pair_at(1 if d == 0 else -1, member))

    def line_sends(d, s):
        onward = pair < pairs - 1 if d == 0 else pair > 0
        return onward & line_exists(d, s - 1)

    def line_start(p, u):
        for d in range(2):

            @pl.when(line_sends(d, 1))
            def _(d=d):
                line_copy(p, d, 1, u).start()

    def line_step(p, s, u, last=False):
        for d in range(2):

            @pl.when(line_exists(d, s))
            def _(d=d):
                ref = in_sub(p, pair - s if d == 0 else pair + s, u)
                line_ref_copy(p, d, s, u, ref, pair_at(-1 if d == 0 else 1, member)).wait_recv()

            if not last:

                @pl.when(line_sends(d, s + 1))
                def _(d=d):
                    line_copy(p, d, s + 1, u).start()

    def line_middle(p):
        def step(s, carry):
            for u in range(2):
                line_step(p, s, u)
            return carry

        lax.fori_loop(3, pairs - 1, step, 0)

    def line_sent():
        def step(s, carry):
            for p in range(2):
                for u in range(2):
                    for d in range(2):

                        @pl.when(line_sends(d, s))
                        def _(p=p, d=d, u=u):
                            line_copy(p, d, s, u).wait_send()

            return carry

        lax.fori_loop(1, pairs, step, 0)

    out_rows = pool_ch + q_width

    def out_sub(owner, u):
        if wide:
            return out_w.at[owner, u]
        return out_w.at[owner, 0, pl.ds(u * (out_rows // SUBS), out_rows // SUBS)]

    def ring_copy(sub, sems, d, s, u):
        owner = owner_at(place - (s - 1) if d == 0 else place + (s - 1))
        ref = sub(owner, u)
        return pltpu.make_async_remote_copy(
            src_ref=ref,
            dst_ref=ref,
            send_sem=sems[0].at[d, s - 1, u],
            recv_sem=sems[1].at[d, s - 1, u],
            device_id=ahead if d == 0 else behind,
            device_id_type=MESH,
        )

    def ring_arrived(sub, sems, d, s, u):
        owner = owner_at(place - s if d == 0 else place + s)
        ref = sub(owner, u)
        pltpu.make_async_remote_copy(
            src_ref=ref,
            dst_ref=ref,
            send_sem=sems[0].at[d, s - 1, u],
            recv_sem=sems[1].at[d, s - 1, u],
            device_id=behind if d == 0 else ahead,
            device_id_type=MESH,
        ).wait_recv()

    ow_ring = (out_sub, (ow_send, ow_recv))

    def ring_start(ring, subs):
        for u in subs:
            for d in range(2):
                ring_copy(*ring, d, 1, u).start()

    def in_half(d, u):
        return u < SUBS // 2 if d == 0 else u >= SUBS // 2

    def ring_step(ring, s, u, last):
        for d in range(2):
            ring_arrived(*ring, d, s, u)
            if not last or in_half(d, u):
                ring_copy(*ring, d, s + 1, u).start()

    def ring_last(ring, k):
        ring_arrived(*ring, 0, half, k)
        ring_arrived(*ring, 1, half, SUBS // 2 + k)

    def ring_sent(ring):
        def full(s, carry):
            for u in range(SUBS):
                for d in range(2):
                    ring_copy(*ring, d, s, u).wait_send()
            return carry

        lax.fori_loop(1, half, full, 0)
        for u in range(SUBS):
            ring_copy(*ring, 0 if in_half(0, u) else 1, half, u).wait_send()

    chunk = rows // CHUNKS

    def tok_set(other):
        return 1 - member if other else member

    def tok_rows(other, slot, j):
        return tok.at[tok_set(other), slot, pl.ds(j * chunk, chunk)]

    def tok_copy(other, slot, j, sems, at, target):
        ref = tok_rows(other, slot, j)
        return pltpu.make_async_remote_copy(
            src_ref=ref,
            dst_ref=ref,
            send_sem=sems[0].at[at],
            recv_sem=sems[1].at[at],
            device_id=target,
            device_id_type=MESH,
        )

    def over_chips(other, rel, j, slot):
        return tok_copy(other, slot, j, (tx_send, tx_recv), (int(other), rel - 1, j), chip_peer(rel))

    def over_cores(other, rel, j, slot):
        return tok_copy(other, slot, j, (td_send, td_recv), (int(other), rel, j), partner)

    def over_pair(j, other):
        return tok_copy(other, tp, j, (ty_send, ty_recv), (j,), mate)

    def spread_tokens(other, j):
        for rel in range(1, chips):
            over_chips(other, rel, j, tp).start()
        over_cores(other, 0, j, tp).start()

    pl.semaphore_wait(barrier, len(greeted))
    for which in range(2):

        @pl.when(member == which)
        def _(which=which):
            for copy in own_load(which) + mate_load(1 - which):
                copy.wait()

    for p in range(2):
        mate_weights(p).start()
    line_start(0, 0)
    loads[0].wait()
    for j in range(CHUNKS):
        spread_tokens(False, j)
        over_pair(j, False).start()
    acc[...] = jnp.zeros_like(acc)
    for copy in loads[1:]:
        copy.wait()

    @pl.when(sp == 0)
    def _():
        kv[:, pl.ds(0, WINDOW)] = jnp.zeros((2, WINDOW, kv_width), kv.dtype)
        pool_pad[:, pl.ds(0, POOL_PAD)] = jnp.zeros((2, POOL_PAD, pool_half), pool_pad.dtype)

    @pl.when(sp == n_sp - 1)
    def _():
        kv[:, pl.ds(WINDOW + rows, WINDOW)] = jnp.zeros((2, WINDOW, kv_width), kv.dtype)
        pool_pad[:, pl.ds(POOL_PAD + rows, POOL_PAD)] = jnp.zeros((2, POOL_PAD, pool_half), pool_pad.dtype)

    def take_mate(j):
        over_pair(j, True).wait_recv()
        spread_tokens(True, j)

    def pass_tokens(other, j):
        for rel in range(1, chips):
            over_chips(other, rel, j, source_slot(rel)).wait_recv()
            over_cores(other, rel, j, source_slot(rel)).start()

    norm_rows = 32

    def normalise(other, j):
        for rel in range(chips):
            slot = source_slot(rel)
            over_cores(other, rel, j, (slot // 2) * 2 + 1 - core).wait_recv()
            over_cores(other, rel, j, slot).wait_send()
            if rel:
                over_chips(other, rel, j, tp).wait_send()
        if not other:
            over_pair(j, False).wait_send()
        which = tok_set(other)

        def tile(i, carry):
            at = pl.ds(pl.multiple_of(j * chunk + i * norm_rows, norm_rows), norm_rows)
            total = jnp.zeros((norm_rows, 1), jnp.float32)
            for slot in range(n_tp):
                floats = tok[which, slot, at, :].astype(jnp.float32)
                total = total + jnp.sum(floats * floats, axis=-1, keepdims=True)
            scale = lax.rsqrt(total / (feats * n_tp) + epsilon)
            for slot in range(n_tp):
                floats = tok[which, slot, at, :].astype(jnp.float32)
                tok[which, slot, at, :] = ((floats * scale) * gain[slot]).astype(jnp.bfloat16)
            return carry

        lax.fori_loop(0, chunk // norm_rows, tile, 0)

    def project(other, p, first_chunk, last_chunk, near=True, far=True):
        which = tok_set(other)
        deep = 2 * depth

        def step(k, carry):
            j, owner = first_chunk + k // pairs, k % pairs

            def add():
                at = pl.ds(pl.multiple_of(j * chunk, chunk), chunk)
                offset = owner * deep
                part = tok[which, offset // feats, at, pl.ds(pl.multiple_of(offset % feats, deep), deep)]
                weight = in_w[p][pl.ds(owner * 2, 2)].reshape(deep, -1)
                acc[which, at, pass_cols[p]] += jnp.dot(part, weight, preferred_element_type=jnp.float32)

            if near and far:
                add()
            else:
                distant = jnp.abs(owner - pair) == pairs - 1
                pl.when(distant if far else jnp.logical_not(distant))(add)
            return carry

        lax.fori_loop(0, (last_chunk - first_chunk) * pairs, step, 0)

    lane = lax.broadcasted_iota(jnp.int32, (GRID_W, LANES), 1)
    take_next = (lane % (HEAD_DIM // 2)) < HEAD_DIM // 4

    def turn(other, p, first_chunk, last_chunk):
        which = tok_set(other)

        def pool_tile(i, carry):
            at = pl.ds(pl.multiple_of(i * GRID_W, GRID_W), GRID_W)
            pool_in = acc[which, at, pl.ds(0, pool_half)].astype(jnp.bfloat16)
            stage_pool[which, at, :] = pool_in
            if not other:
                to = pl.ds(pl.multiple_of(POOL_PAD + i * GRID_W, POOL_PAD), GRID_W)
                pool_pad[member, to, :] = pool_in
            return carry

        def head_tile(i, carry):
            at = pl.ds(pl.multiple_of(i * GRID_W, GRID_W), GRID_W)
            grid_row = (pair * 2 + which) * (rows // GRID_W) + i
            cosine = row_cos[pl.ds(grid_row, 1), :] + col_cos[...]
            sine = row_sin[pl.ds(grid_row, 1), :] + col_sin[...]

            def turned(start):
                raw = acc[which, at, pl.ds(start, LANES)]
                moved = jnp.where(
                    take_next,
                    pltpu.roll(raw, LANES - HEAD_DIM // 4, 1),
                    pltpu.roll(raw, HEAD_DIM // 4, 1),
                )
                return raw, raw * cosine + moved * sine

            for slab in range(q_half // LANES):
                _, values = turned(pool_half + slab * LANES)
                values = (values * HEAD_DIM ** (-0.5)).astype(jnp.bfloat16)
                if other:
                    stage_q[at, pl.ds(slab * LANES, LANES)] = values
                else:
                    queries[member, at, pl.ds(slab * LANES, LANES)] = values
            raw, values = turned(pool_half + q_half)
            values = jnp.where(member == 0, values, raw).astype(jnp.bfloat16)
            stage_kv[which, at, :] = values
            if not other:
                to = pl.ds(pl.multiple_of(WINDOW + i * GRID_W, GRID_W), GRID_W)
                kv[member, to, :] = values
            return carry

        per_chunk = chunk // GRID_W
        lax.fori_loop(first_chunk * per_chunk, last_chunk * per_chunk, pool_tile if p else head_tile, 0)

    def swap(p, j, kind):
        at = pl.ds(j * chunk, chunk)
        return [
            pltpu.make_async_remote_copy(
                src_ref=src,
                dst_ref=dst,
                send_sem=swap_send.at[k, j],
                recv_sem=swap_recv.at[k, j],
                device_id=mate,
                device_id_type=MESH,
            )
            for k, (src, dst) in enumerate(
                (
                    (stage_kv.at[1 - member, at], kv.at[kind, pl.ds(WINDOW + j * chunk, chunk)]),
                    (stage_q.at[at], queries.at[kind, at]),
                    (stage_pool.at[1 - member, at], pool_pad.at[kind, pl.ds(POOL_PAD + j * chunk, chunk)]),
                )
            )
            if (k == 2) == (p == 1)
        ]

    halo_parts = ((stage_kv, kv, WINDOW), (stage_pool, pool_pad, POOL_PAD))

    def halo(k, kind, route):
        stage, held, width = halo_parts[k]
        top, low = pl.ds(rows - width, width), pl.ds(0, width)
        if route == 0:
            first = pl.ds(pl.multiple_of((1 - member) * (rows - width), width), width)
            to = pl.ds(pl.multiple_of(member * (rows + width), width), width)
            src, dst, target = stage.at[member, first], held.at[kind, to], mate
        elif route == 1:
            src, dst, target = stage.at[1, top], held.at[kind, low], pair_at(1, 0)
        else:
            src, dst, target = stage.at[0, low], held.at[kind, pl.ds(rows + width, width)], pair_at(-1, 1)
        return pltpu.make_async_remote_copy(
            src_ref=src,
            dst_ref=dst,
            send_sem=halo_send.at[k, kind, route],
            recv_sem=halo_recv.at[k, kind, route],
            device_id=target,
            device_id_type=MESH,
        )

    def each_member(body):
        for which in range(2):

            @pl.when(member == which)
            def _(which=which):
                body(which)

    kind_cols = 2 * heads_kv * LANES

    def spread_rows(start, count):
        at = pl.ds(start, count)
        for kind in range(2):
            kvx[at, pl.ds(kind * kind_cols, kind_cols)] = jnp.dot(
                kv[kind, at, :], spread[...], preferred_element_type=jnp.float32
            ).astype(jnp.bfloat16)

    span = 3 * WINDOW
    group = Q_HEADS // KV_HEADS
    blocks = rows // WINDOW

    def variant(kind, head, upper):
        return pl.ds(((kind * heads_kv + head) * 2 + upper) * LANES, LANES)

    def attend(i, carry):
        at = pl.ds(pl.multiple_of(i * WINDOW, WINDOW), WINDOW)
        keys_at = pl.ds(pl.multiple_of(i * WINDOW, WINDOW), span)
        query = lax.broadcasted_iota(jnp.int32, (WINDOW, span), 0)
        key = lax.broadcasted_iota(jnp.int32, (WINDOW, span), 1)
        low = jnp.where((sp == 0) & (i == 0), WINDOW, 0)
        high = jnp.where((sp == n_sp - 1) & (i == blocks - 1), 2 * WINDOW, span)
        allowed = (key >= jnp.maximum(query, low)) & (key <= jnp.minimum(query + 2 * WINDOW, high - 1))
        slabs_half = q_half // LANES
        for head in range(heads_kv):
            for two in range(group // 2):
                slab = head * (group // 2) + two
                q_pair = queries[slab // slabs_half, at, pl.ds((slab % slabs_half) * LANES, LANES)]
                result = jnp.zeros((WINDOW, LANES), jnp.float32)
                for upper in range(2):
                    scores = lax.dot_general(
                        q_pair,
                        kvx[keys_at, variant(0, head, upper)],
                        (((1,), (1,)), ((), ())),
                        preferred_element_type=jnp.float32,
                    )
                    scores = jnp.where(allowed, scores, masked_score)
                    logit = sink[slab * 2 + upper]
                    highest = jnp.maximum(jnp.max(scores, axis=-1, keepdims=True), logit)
                    expo = jnp.exp(scores - highest)
                    denominator = jnp.sum(expo, axis=-1, keepdims=True) + jnp.exp(logit - highest)
                    weights = (expo * (1.0 / denominator)).astype(jnp.bfloat16)
                    result += jnp.dot(
                        weights, kvx[keys_at, variant(1, head, upper)], preferred_element_type=jnp.float32
                    )
                mixers[at, pl.ds(pool_ch + slab * LANES, LANES)] = result.astype(jnp.bfloat16)
        return carry

    per_chunk = chunk // WINDOW

    def attend_chunk(j):
        each_member(lambda which: [copy.wait_recv() for copy in swap(0, j, 1 - which)])
        for b in range(per_chunk):
            spread_rows(WINDOW + (j * per_chunk + b) * WINDOW, WINDOW)
        lax.fori_loop(max(1, j * per_chunk - 1), (j + 1) * per_chunk - 1, attend, 0)

    mate_weights(0).wait_recv()
    line_start(0, 1)
    line_step(0, 1, 0)
    pass_tokens(False, 0)
    line_step(0, 1, 1)
    normalise(False, 0)
    pass_tokens(False, 1)
    take_mate(0)
    line_step(0, 2, 0)
    normalise(False, 1)
    line_step(0, 2, 1)
    line_middle(0)
    mate_weights(1).wait_recv()
    for u in range(2):
        line_start(1, u)
    pass_tokens(False, 2)
    take_mate(1)
    normalise(False, 2)
    line_step(0, pairs - 1, 0, True)
    pass_tokens(False, 3)
    take_mate(2)
    line_step(0, pairs - 1, 1, True)
    normalise(False, 3)

    def mate_chunk(p, j, near=True):
        project(True, p, j, j + 1, near=near)
        turn(True, p, j, j + 1)
        each_member(lambda which: [copy.start() for copy in swap(p, j, which)])

    at_end = (pair == 0) | (pair == pairs - 1)

    def early_ring(u):
        @pl.when(at_end)
        def _():
            ring_start(ow_ring, (u,))

    pass_tokens(True, 0)
    line_step(1, 1, 0)
    take_mate(3)
    early_ring(0)
    project(False, 0, 0, CHUNKS)
    line_step(1, 1, 1)
    early_ring(1)
    normalise(True, 0)
    mate_chunk(0, 0)
    line_step(1, 2, 0)
    pass_tokens(True, 1)
    line_step(1, 2, 1)
    line_middle(1)

    @pl.when(jnp.logical_not(at_end))
    def _():
        ring_start(ow_ring, range(SUBS))

    early_ring(2)
    normalise(True, 1)
    mate_chunk(0, 1)
    turn(False, 0, 0, CHUNKS)
    early_ring(3)
    project(False, 1, 0, CHUNKS, far=False)
    pass_tokens(True, 2)
    normalise(True, 2)
    mate_chunk(0, 2)
    project(True, 1, 0, CHUNKS - 1, far=False)
    for j in range(CHUNKS - 2):
        attend_chunk(j)
    line_step(1, pairs - 1, 0, True)
    line_step(1, pairs - 1, 1, True)
    for j in range(CHUNKS - 1):
        mate_chunk(1, j, near=False)
    pass_tokens(True, CHUNKS - 1)
    project(False, 1, 0, CHUNKS, near=False)
    turn(False, 1, 0, CHUNKS)
    normalise(True, CHUNKS - 1)
    mate_chunk(0, CHUNKS - 1)
    mate_chunk(1, CHUNKS - 1)

    def halo_starts(which):
        for k in range(2):
            halo(k, which, 0).start()

        @pl.when(pair < pairs - 1)
        def _():
            for k in range(2):
                halo(k, which, 1).start()

        @pl.when(pair > 0)
        def _():
            for k in range(2):
                halo(k, which, 2).start()

    each_member(halo_starts)

    @pl.when(member == 0)
    def _():
        for stage, held, width in halo_parts:
            held[0, pl.ds(rows + width, width)] = stage[1, pl.ds(0, width)]

    @pl.when(member == 1)
    def _():
        for stage, held, width in halo_parts:
            held[1, pl.ds(0, width)] = stage[0, pl.ds(rows - width, width)]

    ring_step(ow_ring, 1, 0, False)
    attend_chunk(CHUNKS - 2)
    ring_step(ow_ring, 1, 1, False)
    attend_chunk(CHUNKS - 1)
    ring_step(ow_ring, 1, 2, False)

    def halo_waits(which):
        for k in range(2):
            halo(k, 1 - which, 0).wait_recv()

        @pl.when(pair > 0 if which == 0 else pair < pairs - 1)
        def _():
            for k in range(2):
                for kind in range(2):
                    halo(k, kind, 1 if which == 0 else 2).wait_recv()

    each_member(halo_waits)
    spread_rows(0, WINDOW)
    spread_rows(WINDOW + rows, WINDOW)
    lax.fori_loop(0, 2, lambda e, carry: attend(e * (blocks - 1), carry), 0)

    each_member(lambda which: [copy.wait_recv() for j in range(CHUNKS) for copy in swap(1, j, 1 - which)])

    groups_dev = pool_ch // GROUP_DIM
    tile_rows = 256

    def pool_tile(i, carry):
        at = pl.ds(pl.multiple_of(i * tile_rows, tile_rows), tile_rows)
        span_rows = tile_rows + 2 * POOL_PAD
        row = lax.broadcasted_iota(jnp.int32, (tile_rows, span_rows), 0)
        rel = lax.broadcasted_iota(jnp.int32, (tile_rows, span_rows), 1) - POOL_PAD - row
        position = sp * rows + i * tile_rows + lax.broadcasted_iota(jnp.int32, (tile_rows, LANES), 0)
        for g in range(groups_dev):
            level = (tp * groups_dev + g) % 4
            reach = jnp.where(level == 0, 1, jnp.where(level == 1, 2, jnp.where(level == 2, 4, 8)))
            band = jnp.where((rel >= -reach) & (rel < reach), 1.0, 0.0).astype(jnp.bfloat16)
            cols = pl.ds(g * GROUP_DIM, GROUP_DIM)

            def pool_rows(at_rows):
                if pool_half >= GROUP_DIM:
                    begin = g * GROUP_DIM
                    return pool_pad[begin // pool_half, at_rows, pl.ds(begin % pool_half, GROUP_DIM)]
                return jnp.concatenate([pool_pad[0, at_rows, :], pool_pad[1, at_rows, :]], axis=1)

            around = pool_rows(pl.ds(pl.multiple_of(i * tile_rows, tile_rows), span_rows))
            here = pool_rows(pl.ds(pl.multiple_of(i * tile_rows + POOL_PAD, POOL_PAD), tile_rows))
            window_sum = jnp.dot(band, around, preferred_element_type=jnp.float32)
            count = jnp.minimum(position + reach, n_sp * rows) - jnp.maximum(position - reach, 0)
            count = jnp.concatenate([count.astype(jnp.float32)] * (GROUP_DIM // LANES), axis=1)
            pooled = (window_sum / count - here.astype(jnp.float32)).astype(jnp.bfloat16)
            mixed = jnp.dot(pooled, pool_w[g], preferred_element_type=jnp.float32)
            mixers[at, cols] = (mixed * pool_scale[:, cols]).astype(jnp.bfloat16)
        return carry

    lax.fori_loop(0, rows // tile_rows, pool_tile, 0)
    ring_step(ow_ring, 1, 3, False)

    def piece_at(m):
        later = m - nq
        s = later // (2 * nq) + 1
        r = later - (s - 1) * (2 * nq)
        final = s == half
        q = jnp.where(final, r, r // 2)
        delta = jnp.where(final | (r % 2 == 0), -s, s)
        own = m < nq
        return owner_at(place + jnp.where(own, 0, delta)), jnp.where(own, m, q)

    def weight_quarters(m, q):
        final = m >= pieces - nq
        return jnp.where(final, q, 2 * q), jnp.where(final, q + SUBS // 2, 2 * q + 1)

    def core_copy(m, rel):
        c = (chip + rel) % chips
        return pltpu.make_async_remote_copy(
            src_ref=to_core.at[m, c],
            dst_ref=from_core.at[m, c],
            send_sem=core_send.at[m, rel],
            recv_sem=core_recv.at[m, rel],
            device_id=partner,
            device_id_type=MESH,
        )

    def chip_copy(m, rel):
        return pltpu.make_async_remote_copy(
            src_ref=own_sum.at[m, (chip + rel) % chips],
            dst_ref=from_chip.at[m, rel - 1],
            send_sem=chip_send.at[m, rel - 1],
            recv_sem=chip_recv.at[m, rel - 1],
            device_id=chip_peer(rel),
            device_id_type=MESH,
        )

    def multiply(m):
        owner, q = piece_at(m)

        def part(k, carry):
            rel = (k // 2 + 1) % chips
            c = (chip + rel) % chips
            mine = jnp.where(k % 2 == 0, 1 - core, core)
            at = pl.ds(pl.multiple_of((2 * c + mine) * part_rows, part_rows), part_rows)
            if wide:
                first, second = weight_quarters(m, q)
                weight = jnp.concatenate([out_w[owner, first], out_w[owner, second]], axis=1)
            else:
                weight = out_w[owner, q]
            result = jnp.dot(mixers[at, :], weight, preferred_element_type=jnp.float32).astype(jnp.bfloat16)

            @pl.when(k % 2 == 0)
            def _():
                to_core[m, c] = result
                core_copy(m, rel).start()

            @pl.when(k % 2 == 1)
            def _():
                own_sum[m, c] = result

            return carry

        lax.fori_loop(0, n_tp, part, 0)

    def pass_sum(m):
        for rel in range(1, chips):
            core_copy(m, rel).wait_recv()
            c = (chip + rel) % chips
            both = own_sum[m, c].astype(jnp.float32) + from_core[m, c].astype(jnp.float32)
            own_sum[m, c] = both.astype(jnp.bfloat16)
            chip_copy(m, rel).start()

    def total(m):
        owner, q = piece_at(m)
        core_copy(m, 0).wait_recv()
        value = own_sum[m, chip].astype(jnp.float32) + from_core[m, chip].astype(jnp.float32)
        for rel in range(1, chips):
            chip_copy(m, rel).wait_recv()
            value = value + from_chip[m, rel - 1].astype(jnp.float32)
        value = value.astype(out.dtype)
        if wide:
            for k, quarter in enumerate(weight_quarters(m, q)):
                to = pl.ds(pl.multiple_of(owner * cols_dev + quarter * col_w, col_w), col_w)
                out[:, to] = value[:, k * col_w : (k + 1) * col_w]
        else:
            out[:, pl.ds(pl.multiple_of(owner * cols_dev, cols_dev), cols_dev)] = value

    def piece(m, carry):
        multiply(m)
        pass_sum(m)

        @pl.when(m >= LAG)
        def _():
            total(m - LAG)

        return carry

    lax.fori_loop(0, 3 * nq, piece, 0)

    def out_step(s, last):
        for u in range(SUBS):
            ring_step(ow_ring, s, u, last)
            if (u + 1) % nr == 0:
                first = nq + (s - 1) * 2 * nq + 2 * (u // nr)
                lax.fori_loop(first, first + 2, piece, 0)

    def middle_out(s, carry):
        out_step(s, False)
        return carry

    lax.fori_loop(2, half - 1, middle_out, 0)
    out_step(half - 1, True)
    for k in range(SUBS // 2):
        ring_last(ow_ring, k)
        if wide:
            lax.fori_loop(pieces - nq + k, pieces - nq + k + 1, piece, 0)
    if not wide:
        lax.fori_loop(pieces - nq, pieces, piece, 0)

    def finish(m, carry):
        total(m)
        return carry

    lax.fori_loop(pieces - LAG, pieces, finish, 0)

    line_sent()
    ring_sent(ow_ring)
    for p in range(2):
        mate_weights(p).wait_send()

    def pair_sent(which):
        for j in range(CHUNKS):
            for copy in swap(0, j, which) + swap(1, j, which):
                copy.wait_send()
        for k in range(2):
            halo(k, which, 0).wait_send()

        @pl.when(pair < pairs - 1)
        def _():
            for k in range(2):
                halo(k, which, 1).wait_send()

        @pl.when(pair > 0)
        def _():
            for k in range(2):
                halo(k, which, 2).wait_send()

    each_member(pair_sent)

    def sums_sent(m, carry):
        core_copy(m, 0).wait_send()
        for rel in range(1, chips):
            core_copy(m, rel).wait_send()
            chip_copy(m, rel).wait_send()
        return carry

    lax.fori_loop(0, pieces, sums_sent, 0)


def shards(
    n_sp,
    n_tp,
    tokens,
    norm_gain,
    pool_in_weight,
    query_weight,
    key_weight,
    value_weight,
    pool_weight,
    pool_scale,
    sink_logit,
    out_pool_weight,
    out_attn_weight,
):
    rows, feats = tokens.shape
    depth, pool_ch = pool_in_weight.shape
    q_width = query_weight.shape[1]
    kvw = key_weight.shape[1]
    cols_dev = out_pool_weight.shape[1]
    pool_half, q_half = pool_ch // 2, q_width // 2
    out_rows = pool_ch + q_width
    half = n_sp // 2
    chips = n_tp // 2
    wide = cols_dev == SUBS * LANES
    nq = SUBS // 2 if wide else 1
    col_q = cols_dev // nq
    pieces = n_sp * nq
    part_rows = rows // n_tp
    kv_width = -(-kvw // LANES) * LANES
    in_cols = pool_half + q_half + kv_width
    if kv_width != kvw:
        key_weight, value_weight = (jnp.pad(w, ((0, 0), (0, kv_width - kvw))) for w in (key_weight, value_weight))
    tables = [jnp.asarray(t) for t in rotary_tables(rows * n_sp)]
    spread = jnp.asarray(spread_matrix(kvw // HEAD_DIM, kv_width), jnp.bfloat16)
    dims = dict(sp=n_sp, tp=n_tp, heads_kv=kvw // HEAD_DIM, nq=nq, wide=wide)
    small = (norm_gain.reshape(n_tp, 1, feats), pool_weight, pool_scale.reshape(1, pool_ch), *tables, spread)

    def kernel(*refs):
        layer_kernel(dims, *refs[:7], refs[7 : 7 + len(small)], *refs[7 + len(small) :])

    anywhere = pl.BlockSpec(memory_space=pl.ANY)
    vmem = pl.BlockSpec(memory_space=pltpu.VMEM)
    smem = pl.BlockSpec(memory_space=pltpu.SMEM)
    bf16, f32, dma = jnp.bfloat16, jnp.float32, pltpu.SemaphoreType.DMA
    return pl.pallas_call(
        kernel,
        out_shape=pltpu.VMEM((rows // n_tp, cols_dev * n_sp), bf16),
        in_specs=[anywhere] * (7 + len(small)) + [smem],
        out_specs=vmem,
        scratch_shapes=[
            pltpu.VMEM((2, n_tp, rows, feats), bf16),
            pltpu.VMEM((n_sp, depth, q_half + kv_width), bf16),
            pltpu.VMEM((n_sp, depth, pool_half), bf16),
            pltpu.VMEM((depth, q_half + kv_width), bf16),
            pltpu.VMEM((depth, pool_half), bf16),
            pltpu.VMEM((n_sp, SUBS if wide else 1, out_rows, LANES if wide else cols_dev), bf16),
            pltpu.VMEM((2, rows, in_cols), f32),
            pltpu.VMEM((2, rows, q_half), bf16),
            pltpu.VMEM((2, rows + 2 * POOL_PAD, pool_half), bf16),
            pltpu.VMEM((2, rows + 2 * WINDOW, kv_width), bf16),
            pltpu.VMEM((2, rows, pool_half), bf16),
            pltpu.VMEM((rows, q_half), bf16),
            pltpu.VMEM((2, rows, kv_width), bf16),
            pltpu.VMEM((rows + 2 * WINDOW, 4 * (kvw // HEAD_DIM) * LANES), bf16),
            pltpu.VMEM((rows, out_rows), bf16),
            pltpu.VMEM((pieces, chips, part_rows, col_q), bf16),
            pltpu.VMEM((pieces, chips, part_rows, col_q), bf16),
            pltpu.VMEM((pieces, chips, part_rows, col_q), bf16),
            pltpu.VMEM((pieces, chips - 1, part_rows, col_q), bf16),
            *[pltpu.VMEM(value.shape, value.dtype) for value in small],
            dma((7 + 2 * (SUBS if wide else 1) + len(small),)),
            dma((2,)),
            dma((2,)),
            dma((2, 2, half, 2)),
            dma((2, 2, half, 2)),
            dma((2, half, SUBS)),
            dma((2, half, SUBS)),
            dma((2, chips - 1, CHUNKS)),
            dma((2, chips - 1, CHUNKS)),
            dma((2, chips, CHUNKS)),
            dma((2, chips, CHUNKS)),
            dma((CHUNKS,)),
            dma((CHUNKS,)),
            dma((3, CHUNKS)),
            dma((3, CHUNKS)),
            dma((2, 2, 3)),
            dma((2, 2, 3)),
            dma((pieces, chips)),
            dma((pieces, chips)),
            dma((pieces, chips - 1)),
            dma((pieces, chips - 1)),
        ],
        compiler_params=pltpu.CompilerParams(
            collective_id=0, has_side_effects=True, vmem_limit_bytes=61 * 2**20
        ),
        name="layer",
    )(
        tokens,
        pool_in_weight,
        query_weight,
        key_weight,
        value_weight,
        out_pool_weight,
        out_attn_weight,
        *small,
        sink_logit,
    )


def solution(mesh):
    return jax.shard_map(
        functools.partial(shards, mesh.shape["sp"], mesh.shape["tp"]),
        mesh=mesh,
        in_specs=(
            P("sp", "tp"),
            P(),
            P("sp", "tp"),
            P("sp", "tp"),
            P("sp", "tp"),
            P("sp", "tp"),
            P("tp", None, None),
            P("tp"),
            P("tp"),
            P("tp", "sp"),
            P("tp", "sp"),
        ),
        out_specs=P(("sp", "tp"), None),
        check_vma=False,
    )
```

```python
import functools

import jax
import jax.numpy as jnp
import numpy as np
from jax import lax
from jax.experimental import pallas as pl
from jax.experimental.pallas import tpu as pltpu
from jax.sharding import PartitionSpec as P

HEAD_DIM = 64
Q_HEADS = 32
KV_HEADS = 8
GROUP_DIM = 256
WINDOW = 128
GRID_W = 64
LANES = 128
SUBS = 4
CHUNKS = 4
POOL_PAD = 16
LAG = 3

epsilon = 1e-06
rotary_base = 10000.0
masked_score = -1e30
MESH = pl.DeviceIdType.MESH


def rotary_tables(total_rows):
    freq_count = HEAD_DIM // 4
    inverse = np.float32(rotary_base) ** (-np.arange(freq_count, dtype=np.float32) / np.float32(freq_count))
    lane = np.arange(LANES)
    dim = lane % HEAD_DIM
    by_col = (dim // (HEAD_DIM // 2)) == 1
    is_b = (dim % (HEAD_DIM // 2)) // freq_count == 1
    freq = inverse[dim % freq_count]
    sign = np.where(is_b, np.float32(1.0), np.float32(-1.0))
    tables = []
    for count, mine in ((total_rows // GRID_W, ~by_col), (GRID_W, by_col)):
        angle = np.arange(count, dtype=np.float32)[:, None] * freq[None, :]
        tables.append(np.where(mine, np.cos(angle), np.float32(0.0)).astype(np.float32))
        tables.append(np.where(mine, np.sin(angle) * sign, np.float32(0.0)).astype(np.float32))
    return tables


def spread_matrix(heads, width):
    spread = np.zeros((width, 2 * heads * LANES), np.float32)
    for head in range(heads):
        for half in range(2):
            for d in range(HEAD_DIM):
                spread[head * HEAD_DIM + d, (head * 2 + half) * LANES + half * HEAD_DIM + d] = 1.0
    return spread


def layer_kernel(
    dims,
    tokens,
    pool_in_w,
    query_w,
    key_w,
    value_w,
    out_pool_w,
    out_attn_w,
    small_refs,
    sink,
    out,
    tok,
    in_a,
    in_b,
    mate_a,
    mate_b,
    out_w,
    acc,
    queries,
    pool_pad,
    kv,
    stage_pool,
    stage_q,
    stage_kv,
    kvx,
    mixers,
    to_core,
    own_sum,
    from_core,
    from_chip,
    gain,
    pool_w,
    pool_scale,
    row_cos,
    row_sin,
    col_cos,
    col_sin,
    spread,
    load_sem,
    pw_send,
    pw_recv,
    in_send,
    in_recv,
    ow_send,
    ow_recv,
    tx_send,
    tx_recv,
    td_send,
    td_recv,
    ty_send,
    ty_recv,
    swap_send,
    swap_recv,
    halo_send,
    halo_recv,
    core_send,
    core_recv,
    chip_send,
    chip_recv,
):
    n_sp, n_tp = dims["sp"], dims["tp"]
    rows, feats = tokens.shape
    depth = pool_in_w.shape[0]
    pool_ch = pool_in_w.shape[1]
    q_width = query_w.shape[1]
    heads_kv = dims["heads_kv"]
    kv_width = key_w.shape[1]
    pool_half = pool_ch // 2
    q_half = q_width // 2
    cols_dev = out_pool_w.shape[1]
    nq = dims["nq"]
    wide = dims["wide"]
    nr = SUBS // nq
    col_q = cols_dev // nq
    half = n_sp // 2
    chips = n_tp // 2
    part_rows = rows // n_tp
    pieces = n_sp * nq

    sp = lax.axis_index("sp")
    tp = lax.axis_index("tp")
    chip = tp // 2
    core = tp % 2
    place = jnp.where(sp % 2 == 0, sp // 2, n_sp - 1 - sp // 2)
    pairs = n_sp // 2
    pair = sp // 2
    member = sp % 2
    mate = (pair * 2 + 1 - member, tp)

    def pair_at(offset, which):
        return (((pair + offset + pairs) % pairs) * 2 + which, tp)

    def owner_at(spot):
        spot = (spot + n_sp) % n_sp
        return jnp.where(spot < half, 2 * spot, 2 * (n_sp - 1 - spot) + 1)

    ahead = (owner_at(place + 1), tp)
    behind = (owner_at(place - 1), tp)
    partner = (sp, chip * 2 + 1 - core)

    def chip_peer(rel):
        return (sp, ((chip + rel) % chips) * 2 + core)

    def source_slot(rel):
        return ((chip - rel + chips) % chips) * 2 + core

    barrier = pltpu.get_barrier_semaphore()
    greeted = [ahead, behind, mate, partner]
    greeted += [pair_at(offset, which) for offset in (1, -1) for which in (member, 1 - member)]
    greeted += [chip_peer(rel) for rel in range(1, chips)]
    for other in greeted:
        pl.semaphore_signal(barrier, inc=1, device_id=other, device_id_type=MESH)

    loads = []

    def load(src, dst):
        copy = pltpu.make_async_copy(src, dst, load_sem.at[6 + len(loads)])
        copy.start()
        loads.append(copy)

    in_w = (in_a, in_b)

    def local_loads(which, heads_to, pool_to, first):
        parts = (
            (query_w.at[:, pl.ds(which * q_half, q_half)], heads_to.at[:, pl.ds(0, q_half)]),
            (key_w if which == 0 else value_w, heads_to.at[:, pl.ds(q_half, kv_width)]),
            (pool_in_w.at[:, pl.ds(which * pool_half, pool_half)], pool_to),
        )
        return [pltpu.make_async_copy(src, dst, load_sem.at[first + k]) for k, (src, dst) in enumerate(parts)]

    def own_load(which):
        return local_loads(which, in_a.at[sp], in_b.at[sp], 0)

    def mate_load(which):
        return local_loads(which, mate_a, mate_b, 3)

    def mate_weights(p):
        return pltpu.make_async_remote_copy(
            src_ref=(mate_a, mate_b)[p],
            dst_ref=in_w[p].at[sp],
            send_sem=pw_send.at[p],
            recv_sem=pw_recv.at[p],
            device_id=mate,
            device_id_type=MESH,
        )

    for which in range(2):

        @pl.when(member == which)
        def _(which=which):
            for copy in own_load(which) + mate_load(1 - which):
                copy.start()

    load(tokens, tok.at[member, tp])
    quarters = SUBS if wide else 1
    col_w = cols_dev // quarters
    for q in range(quarters):
        load(out_pool_w.at[:, pl.ds(q * col_w, col_w)], out_w.at[sp, q, pl.ds(0, pool_ch)])
        load(out_attn_w.at[:, pl.ds(q * col_w, col_w)], out_w.at[sp, q, pl.ds(pool_ch, q_width)])
    for src, dst in zip(small_refs, (gain, pool_w, pool_scale, row_cos, row_sin, col_cos, col_sin, spread)):
        load(src, dst)

    pass_cols = (pl.ds(pool_half, q_half + kv_width), pl.ds(0, pool_half))

    def in_sub(p, which_pair, u):
        owner = which_pair * 2 + (member if u == 0 else 1 - member)
        return in_w[p].at[owner]

    def line_exists(d, s):
        return pair >= s if d == 0 else pair < pairs - s

    def line_ref_copy(p, d, s, u, ref, target):
        return pltpu.make_async_remote_copy(
            src_ref=ref,
            dst_ref=ref,
            send_sem=in_send.at[p, d, s - 1, u],
            recv_sem=in_recv.at[p, d, s - 1, u],
            device_id=target,
            device_id_type=MESH,
        )

    def line_copy(p, d, s, u):
        ref = in_sub(p, pair - (s - 1) if d == 0 else pair + (s - 1), u)
        return line_ref_copy(p, d, s, u, ref, pair_at(1 if d == 0 else -1, member))

    def line_sends(d, s):
        onward = pair < pairs - 1 if d == 0 else pair > 0
        return onward & line_exists(d, s - 1)

    def line_start(p, u):
        for d in range(2):

            @pl.when(line_sends(d, 1))
            def _(d=d):
                line_copy(p, d, 1, u).start()

    def line_step(p, s, u, last=False):
        for d in range(2):

            @pl.when(line_exists(d, s))
            def _(d=d):
                ref = in_sub(p, pair - s if d == 0 else pair + s, u)
                line_ref_copy(p, d, s, u, ref, pair_at(-1 if d == 0 else 1, member)).wait_recv()

            if not last:

                @pl.when(line_sends(d, s + 1))
                def _(d=d):
                    line_copy(p, d, s + 1, u).start()

    def line_middle(p):
        def step(s, carry):
            for u in range(2):
                line_step(p, s, u)
            return carry

        lax.fori_loop(3, pairs - 1, step, 0)

    def line_sent():
        def step(s, carry):
            for p in range(2):
                for u in range(2):
                    for d in range(2):

                        @pl.when(line_sends(d, s))
                        def _(p=p, d=d, u=u):
                            line_copy(p, d, s, u).wait_send()

            return carry

        lax.fori_loop(1, pairs, step, 0)

    out_rows = pool_ch + q_width

    def out_sub(owner, u):
        if wide:
            return out_w.at[owner, u]
        return out_w.at[owner, 0, pl.ds(u * (out_rows // SUBS), out_rows // SUBS)]

    def ring_copy(sub, sems, d, s, u):
        owner = owner_at(place - (s - 1) if d == 0 else place + (s - 1))
        ref = sub(owner, u)
        return pltpu.make_async_remote_copy(
            src_ref=ref,
            dst_ref=ref,
            send_sem=sems[0].at[d, s - 1, u],
            recv_sem=sems[1].at[d, s - 1, u],
            device_id=ahead if d == 0 else behind,
            device_id_type=MESH,
        )

    def ring_arrived(sub, sems, d, s, u):
        owner = owner_at(place - s if d == 0 else place + s)
        ref = sub(owner, u)
        pltpu.make_async_remote_copy(
            src_ref=ref,
            dst_ref=ref,
            send_sem=sems[0].at[d, s - 1, u],
            recv_sem=sems[1].at[d, s - 1, u],
            device_id=behind if d == 0 else ahead,
            device_id_type=MESH,
        ).wait_recv()

    ow_ring = (out_sub, (ow_send, ow_recv))

    def ring_start(ring, subs):
        for u in subs:
            for d in range(2):
                ring_copy(*ring, d, 1, u).start()

    def in_half(d, u):
        return u < SUBS // 2 if d == 0 else u >= SUBS // 2

    def ring_step(ring, s, u, last):
        for d in range(2):
            ring_arrived(*ring, d, s, u)
            if not last or in_half(d, u):
                ring_copy(*ring, d, s + 1, u).start()

    def ring_last(ring, k):
        ring_arrived(*ring, 0, half, k)
        ring_arrived(*ring, 1, half, SUBS // 2 + k)

    def ring_sent(ring):
        def full(s, carry):
            for u in range(SUBS):
                for d in range(2):
                    ring_copy(*ring, d, s, u).wait_send()
            return carry

        lax.fori_loop(1, half, full, 0)
        for u in range(SUBS):
            ring_copy(*ring, 0 if in_half(0, u) else 1, half, u).wait_send()

    chunk = rows // CHUNKS

    def tok_set(other):
        return 1 - member if other else member

    def tok_rows(other, slot, j):
        return tok.at[tok_set(other), slot, pl.ds(j * chunk, chunk)]

    def tok_copy(other, slot, j, sems, at, target):
        ref = tok_rows(other, slot, j)
        return pltpu.make_async_remote_copy(
            src_ref=ref,
            dst_ref=ref,
            send_sem=sems[0].at[at],
            recv_sem=sems[1].at[at],
            device_id=target,
            device_id_type=MESH,
        )

    def over_chips(other, rel, j, slot):
        return tok_copy(other, slot, j, (tx_send, tx_recv), (int(other), rel - 1, j), chip_peer(rel))

    def over_cores(other, rel, j, slot):
        return tok_copy(other, slot, j, (td_send, td_recv), (int(other), rel, j), partner)

    def over_pair(j, other):
        return tok_copy(other, tp, j, (ty_send, ty_recv), (j,), mate)

    def spread_tokens(other, j):
        for rel in range(1, chips):
            over_chips(other, rel, j, tp).start()
        over_cores(other, 0, j, tp).start()

    pl.semaphore_wait(barrier, len(greeted))
    for which in range(2):

        @pl.when(member == which)
        def _(which=which):
            for copy in own_load(which) + mate_load(1 - which):
                copy.wait()

    for p in range(2):
        mate_weights(p).start()
    line_start(0, 0)
    loads[0].wait()
    for j in range(CHUNKS):
        spread_tokens(False, j)
        over_pair(j, False).start()
    acc[...] = jnp.zeros_like(acc)
    for copy in loads[1:]:
        copy.wait()

    @pl.when(sp == 0)
    def _():
        kv[:, pl.ds(0, WINDOW)] = jnp.zeros((2, WINDOW, kv_width), kv.dtype)
        pool_pad[:, pl.ds(0, POOL_PAD)] = jnp.zeros((2, POOL_PAD, pool_half), pool_pad.dtype)

    @pl.when(sp == n_sp - 1)
    def _():
        kv[:, pl.ds(WINDOW + rows, WINDOW)] = jnp.zeros((2, WINDOW, kv_width), kv.dtype)
        pool_pad[:, pl.ds(POOL_PAD + rows, POOL_PAD)] = jnp.zeros((2, POOL_PAD, pool_half), pool_pad.dtype)

    def take_mate(j):
        over_pair(j, True).wait_recv()
        spread_tokens(True, j)

    def pass_tokens(other, j):
        for rel in range(1, chips):
            over_chips(other, rel, j, source_slot(rel)).wait_recv()
            over_cores(other, rel, j, source_slot(rel)).start()

    norm_rows = 32

    def normalise(other, j):
        for rel in range(chips):
            slot = source_slot(rel)
            over_cores(other, rel, j, (slot // 2) * 2 + 1 - core).wait_recv()
            over_cores(other, rel, j, slot).wait_send()
            if rel:
                over_chips(other, rel, j, tp).wait_send()
        if not other:
            over_pair(j, False).wait_send()
        which = tok_set(other)

        def tile(i, carry):
            at = pl.ds(pl.multiple_of(j * chunk + i * norm_rows, norm_rows), norm_rows)
            total = jnp.zeros((norm_rows, 1), jnp.float32)
            for slot in range(n_tp):
                floats = tok[which, slot, at, :].astype(jnp.float32)
                total = total + jnp.sum(floats * floats, axis=-1, keepdims=True)
            scale = lax.rsqrt(total / (feats * n_tp) + epsilon)
            for slot in range(n_tp):
                floats = tok[which, slot, at, :].astype(jnp.float32)
                tok[which, slot, at, :] = ((floats * scale) * gain[slot]).astype(jnp.bfloat16)
            return carry

        lax.fori_loop(0, chunk // norm_rows, tile, 0)

    def project(other, p, first_chunk, last_chunk, near=True, far=True):
        which = tok_set(other)
        deep = 2 * depth
        size = chunk * (2 if (last_chunk - first_chunk) % 2 == 0 else 1)

        def step(k, carry):
            j, owner = k // pairs, k % pairs

            def add():
                at = pl.ds(pl.multiple_of(first_chunk * chunk + j * size, chunk), size)
                offset = owner * deep
                part = tok[which, offset // feats, at, pl.ds(pl.multiple_of(offset % feats, deep), deep)]
                weight = in_w[p][pl.ds(owner * 2, 2)].reshape(deep, -1)
                acc[which, at, pass_cols[p]] += jnp.dot(part, weight, preferred_element_type=jnp.float32)

            if near and far:
                add()
            else:
                distant = jnp.abs(owner - pair) == pairs - 1
                pl.when(distant if far else jnp.logical_not(distant))(add)
            return carry

        lax.fori_loop(0, (last_chunk - first_chunk) * chunk // size * pairs, step, 0)

    lane = lax.broadcasted_iota(jnp.int32, (GRID_W, LANES), 1)
    take_next = (lane % (HEAD_DIM // 2)) < HEAD_DIM // 4

    def turn(other, p, first_chunk, last_chunk):
        which = tok_set(other)

        def pool_tile(i, carry):
            at = pl.ds(pl.multiple_of(i * GRID_W, GRID_W), GRID_W)
            pool_in = acc[which, at, pl.ds(0, pool_half)].astype(jnp.bfloat16)
            stage_pool[which, at, :] = pool_in
            if not other:
                to = pl.ds(pl.multiple_of(POOL_PAD + i * GRID_W, POOL_PAD), GRID_W)
                pool_pad[member, to, :] = pool_in
            return carry

        def head_tile(i, carry):
            at = pl.ds(pl.multiple_of(i * GRID_W, GRID_W), GRID_W)
            grid_row = (pair * 2 + which) * (rows // GRID_W) + i
            cosine = row_cos[pl.ds(grid_row, 1), :] + col_cos[...]
            sine = row_sin[pl.ds(grid_row, 1), :] + col_sin[...]

            def turned(start):
                raw = acc[which, at, pl.ds(start, LANES)]
                moved = jnp.where(
                    take_next,
                    pltpu.roll(raw, LANES - HEAD_DIM // 4, 1),
                    pltpu.roll(raw, HEAD_DIM // 4, 1),
                )
                return raw, raw * cosine + moved * sine

            for slab in range(q_half // LANES):
                _, values = turned(pool_half + slab * LANES)
                values = (values * HEAD_DIM ** (-0.5)).astype(jnp.bfloat16)
                if other:
                    stage_q[at, pl.ds(slab * LANES, LANES)] = values
                else:
                    queries[member, at, pl.ds(slab * LANES, LANES)] = values
            raw, values = turned(pool_half + q_half)
            values = jnp.where(member == 0, values, raw).astype(jnp.bfloat16)
            stage_kv[which, at, :] = values
            if not other:
                to = pl.ds(pl.multiple_of(WINDOW + i * GRID_W, GRID_W), GRID_W)
                kv[member, to, :] = values
            return carry

        per_chunk = chunk // GRID_W
        lax.fori_loop(first_chunk * per_chunk, last_chunk * per_chunk, pool_tile if p else head_tile, 0)

    def swap(p, j, kind):
        at = pl.ds(j * chunk, chunk)
        return [
            pltpu.make_async_remote_copy(
                src_ref=src,
                dst_ref=dst,
                send_sem=swap_send.at[k, j],
                recv_sem=swap_recv.at[k, j],
                device_id=mate,
                device_id_type=MESH,
            )
            for k, (src, dst) in enumerate(
                (
                    (stage_kv.at[1 - member, at], kv.at[kind, pl.ds(WINDOW + j * chunk, chunk)]),
                    (stage_q.at[at], queries.at[kind, at]),
                    (stage_pool.at[1 - member, at], pool_pad.at[kind, pl.ds(POOL_PAD + j * chunk, chunk)]),
                )
            )
            if (k == 2) == (p == 1)
        ]

    halo_parts = ((stage_kv, kv, WINDOW), (stage_pool, pool_pad, POOL_PAD))

    def halo(k, kind, route):
        stage, held, width = halo_parts[k]
        top, low = pl.ds(rows - width, width), pl.ds(0, width)
        if route == 0:
            first = pl.ds(pl.multiple_of((1 - member) * (rows - width), width), width)
            to = pl.ds(pl.multiple_of(member * (rows + width), width), width)
            src, dst, target = stage.at[member, first], held.at[kind, to], mate
        elif route == 1:
            src, dst, target = stage.at[1, top], held.at[kind, low], pair_at(1, 0)
        else:
            src, dst, target = stage.at[0, low], held.at[kind, pl.ds(rows + width, width)], pair_at(-1, 1)
        return pltpu.make_async_remote_copy(
            src_ref=src,
            dst_ref=dst,
            send_sem=halo_send.at[k, kind, route],
            recv_sem=halo_recv.at[k, kind, route],
            device_id=target,
            device_id_type=MESH,
        )

    def each_member(body):
        for which in range(2):

            @pl.when(member == which)
            def _(which=which):
                body(which)

    kind_cols = 2 * heads_kv * LANES

    def spread_rows(start, count):
        at = pl.ds(start, count)
        for kind in range(2):
            kvx[at, pl.ds(kind * kind_cols, kind_cols)] = jnp.dot(
                kv[kind, at, :], spread[...], preferred_element_type=jnp.float32
            ).astype(jnp.bfloat16)

    span = 3 * WINDOW
    group = Q_HEADS // KV_HEADS
    blocks = rows // WINDOW

    def variant(kind, head, upper):
        return pl.ds(((kind * heads_kv + head) * 2 + upper) * LANES, LANES)

    def attend(i, carry):
        at = pl.ds(pl.multiple_of(i * WINDOW, WINDOW), WINDOW)
        keys_at = pl.ds(pl.multiple_of(i * WINDOW, WINDOW), span)
        query = lax.broadcasted_iota(jnp.int32, (WINDOW, span), 0)
        key = lax.broadcasted_iota(jnp.int32, (WINDOW, span), 1)
        low = jnp.where((sp == 0) & (i == 0), WINDOW, 0)
        high = jnp.where((sp == n_sp - 1) & (i == blocks - 1), 2 * WINDOW, span)
        allowed = (key >= jnp.maximum(query, low)) & (key <= jnp.minimum(query + 2 * WINDOW, high - 1))
        slabs_half = q_half // LANES
        for head in range(heads_kv):
            for two in range(group // 2):
                slab = head * (group // 2) + two
                q_pair = queries[slab // slabs_half, at, pl.ds((slab % slabs_half) * LANES, LANES)]
                result = jnp.zeros((WINDOW, LANES), jnp.float32)
                for upper in range(2):
                    scores = lax.dot_general(
                        q_pair,
                        kvx[keys_at, variant(0, head, upper)],
                        (((1,), (1,)), ((), ())),
                        preferred_element_type=jnp.float32,
                    )
                    scores = jnp.where(allowed, scores, masked_score)
                    logit = sink[slab * 2 + upper]
                    highest = jnp.maximum(jnp.max(scores, axis=-1, keepdims=True), logit)
                    expo = jnp.exp(scores - highest)
                    denominator = jnp.sum(expo, axis=-1, keepdims=True) + jnp.exp(logit - highest)
                    weights = (expo * (1.0 / denominator)).astype(jnp.bfloat16)
                    result += jnp.dot(
                        weights, kvx[keys_at, variant(1, head, upper)], preferred_element_type=jnp.float32
                    )
                mixers[at, pl.ds(pool_ch + slab * LANES, LANES)] = result.astype(jnp.bfloat16)
        return carry

    per_chunk = chunk // WINDOW

    def attend_chunk(j):
        each_member(lambda which: [copy.wait_recv() for copy in swap(0, j, 1 - which)])
        for b in range(per_chunk):
            spread_rows(WINDOW + (j * per_chunk + b) * WINDOW, WINDOW)
        lax.fori_loop(max(1, j * per_chunk - 1), (j + 1) * per_chunk - 1, attend, 0)

    def halo_starts(k, route):
        def start(which):
            def go():
                halo(k, which, route).start()

            if route == 0:
                go()
            else:
                pl.when(pair < pairs - 1 if route == 1 else pair > 0)(go)

        each_member(start)

    mate_weights(0).wait_recv()
    line_start(0, 1)
    line_step(0, 1, 0)
    pass_tokens(False, 0)
    line_step(0, 1, 1)
    normalise(False, 0)
    pass_tokens(False, 1)
    take_mate(0)
    line_step(0, 2, 0)
    normalise(False, 1)
    line_step(0, 2, 1)
    line_middle(0)
    mate_weights(1).wait_recv()
    for u in range(2):
        line_start(1, u)
    pass_tokens(False, 2)
    take_mate(1)
    normalise(False, 2)
    project(False, 0, 0, 2, far=False)
    line_step(0, pairs - 1, 0, True)
    pass_tokens(False, 3)
    take_mate(2)
    project(False, 0, 2, 3, far=False)
    line_step(0, pairs - 1, 1, True)
    normalise(False, 3)
    project(False, 0, 3, 4, far=False)

    def mate_chunk(p, j, near=True):
        project(True, p, j, j + 1, near=near)
        turn(True, p, j, j + 1)
        each_member(lambda which: [copy.start() for copy in swap(p, j, which)])

    at_end = (pair == 0) | (pair == pairs - 1)

    def early_ring(u):
        @pl.when(at_end)
        def _():
            ring_start(ow_ring, (u,))

    early_ring(0)
    pass_tokens(True, 0)
    line_step(1, 1, 0)
    take_mate(3)
    project(False, 0, 0, CHUNKS, near=False)
    line_step(1, 1, 1)
    early_ring(1)
    normalise(True, 0)
    mate_chunk(0, 0)
    line_step(1, 2, 0)
    pass_tokens(True, 1)
    line_step(1, 2, 1)
    line_middle(1)

    @pl.when(jnp.logical_not(at_end))
    def _():
        ring_start(ow_ring, range(SUBS))

    early_ring(2)
    normalise(True, 1)
    mate_chunk(0, 1)
    turn(False, 0, 0, CHUNKS)
    halo_starts(0, 0)
    halo_starts(0, 2)
    early_ring(3)
    project(False, 1, 0, CHUNKS, far=False)
    pass_tokens(True, 2)
    normalise(True, 2)
    mate_chunk(0, 2)
    project(True, 1, 0, CHUNKS - 1, far=False)
    for j in range(CHUNKS - 2):
        attend_chunk(j)
    line_step(1, pairs - 1, 0, True)
    line_step(1, pairs - 1, 1, True)
    for j in range(CHUNKS - 1):
        mate_chunk(1, j, near=False)
    pass_tokens(True, CHUNKS - 1)
    project(False, 1, 0, CHUNKS, near=False)
    turn(False, 1, 0, CHUNKS)
    halo_starts(1, 0)
    halo_starts(1, 2)
    normalise(True, CHUNKS - 1)
    mate_chunk(0, CHUNKS - 1)
    halo_starts(0, 1)
    mate_chunk(1, CHUNKS - 1)
    halo_starts(1, 1)

    @pl.when(member == 0)
    def _():
        for stage, held, width in halo_parts:
            held[0, pl.ds(rows + width, width)] = stage[1, pl.ds(0, width)]

    @pl.when(member == 1)
    def _():
        for stage, held, width in halo_parts:
            held[1, pl.ds(0, width)] = stage[0, pl.ds(rows - width, width)]

    attend_chunk(CHUNKS - 2)
    ring_step(ow_ring, 1, 0, False)
    ring_step(ow_ring, 1, 1, False)
    attend_chunk(CHUNKS - 1)
    ring_step(ow_ring, 1, 2, False)

    def halo_waits(which):
        for k in range(2):
            halo(k, 1 - which, 0).wait_recv()

        @pl.when(pair > 0 if which == 0 else pair < pairs - 1)
        def _():
            for k in range(2):
                for kind in range(2):
                    halo(k, kind, 1 if which == 0 else 2).wait_recv()

    each_member(halo_waits)
    spread_rows(0, WINDOW)
    spread_rows(WINDOW + rows, WINDOW)
    lax.fori_loop(0, 2, lambda e, carry: attend(e * (blocks - 1), carry), 0)

    each_member(lambda which: [copy.wait_recv() for j in range(CHUNKS) for copy in swap(1, j, 1 - which)])

    groups_dev = pool_ch // GROUP_DIM
    tile_rows = 256

    def pool_tile(i, carry):
        at = pl.ds(pl.multiple_of(i * tile_rows, tile_rows), tile_rows)
        span_rows = tile_rows + 2 * POOL_PAD
        row = lax.broadcasted_iota(jnp.int32, (tile_rows, span_rows), 0)
        rel = lax.broadcasted_iota(jnp.int32, (tile_rows, span_rows), 1) - POOL_PAD - row
        position = sp * rows + i * tile_rows + lax.broadcasted_iota(jnp.int32, (tile_rows, LANES), 0)
        for g in range(groups_dev):
            level = (tp * groups_dev + g) % 4
            reach = jnp.where(level == 0, 1, jnp.where(level == 1, 2, jnp.where(level == 2, 4, 8)))
            band = jnp.where((rel >= -reach) & (rel < reach), 1.0, 0.0).astype(jnp.bfloat16)
            cols = pl.ds(g * GROUP_DIM, GROUP_DIM)

            def pool_rows(at_rows):
                if pool_half >= GROUP_DIM:
                    begin = g * GROUP_DIM
                    return pool_pad[begin // pool_half, at_rows, pl.ds(begin % pool_half, GROUP_DIM)]
                return jnp.concatenate([pool_pad[0, at_rows, :], pool_pad[1, at_rows, :]], axis=1)

            around = pool_rows(pl.ds(pl.multiple_of(i * tile_rows, tile_rows), span_rows))
            here = pool_rows(pl.ds(pl.multiple_of(i * tile_rows + POOL_PAD, POOL_PAD), tile_rows))
            window_sum = jnp.dot(band, around, preferred_element_type=jnp.float32)
            count = jnp.minimum(position + reach, n_sp * rows) - jnp.maximum(position - reach, 0)
            count = jnp.concatenate([count.astype(jnp.float32)] * (GROUP_DIM // LANES), axis=1)
            pooled = (window_sum / count - here.astype(jnp.float32)).astype(jnp.bfloat16)
            mixed = jnp.dot(pooled, pool_w[g], preferred_element_type=jnp.float32)
            mixers[at, cols] = (mixed * pool_scale[:, cols]).astype(jnp.bfloat16)
        return carry

    lax.fori_loop(0, rows // tile_rows, pool_tile, 0)
    ring_step(ow_ring, 1, 3, False)

    def piece_at(m):
        later = m - nq
        s = later // (2 * nq) + 1
        r = later - (s - 1) * (2 * nq)
        final = s == half
        q = jnp.where(final, r, r // 2)
        delta = jnp.where(final | (r % 2 == 0), -s, s)
        own = m < nq
        return owner_at(place + jnp.where(own, 0, delta)), jnp.where(own, m, q)

    def weight_quarters(m, q):
        final = m >= pieces - nq
        return jnp.where(final, q, 2 * q), jnp.where(final, q + SUBS // 2, 2 * q + 1)

    def core_copy(m, rel):
        c = (chip + rel) % chips
        return pltpu.make_async_remote_copy(
            src_ref=to_core.at[m, c],
            dst_ref=from_core.at[m, c],
            send_sem=core_send.at[m, rel],
            recv_sem=core_recv.at[m, rel],
            device_id=partner,
            device_id_type=MESH,
        )

    def chip_copy(m, rel):
        return pltpu.make_async_remote_copy(
            src_ref=own_sum.at[m, (chip + rel) % chips],
            dst_ref=from_chip.at[m, rel - 1],
            send_sem=chip_send.at[m, rel - 1],
            recv_sem=chip_recv.at[m, rel - 1],
            device_id=chip_peer(rel),
            device_id_type=MESH,
        )

    def multiply(m):
        owner, q = piece_at(m)

        def part(k, carry):
            rel = (k // 2 + 1) % chips
            c = (chip + rel) % chips
            mine = jnp.where(k % 2 == 0, 1 - core, core)
            at = pl.ds(pl.multiple_of((2 * c + mine) * part_rows, part_rows), part_rows)
            if wide:
                first, second = weight_quarters(m, q)
                weight = jnp.concatenate([out_w[owner, first], out_w[owner, second]], axis=1)
            else:
                weight = out_w[owner, q]
            result = jnp.dot(mixers[at, :], weight, preferred_element_type=jnp.float32).astype(jnp.bfloat16)

            @pl.when(k % 2 == 0)
            def _():
                to_core[m, c] = result
                core_copy(m, rel).start()

            @pl.when(k % 2 == 1)
            def _():
                own_sum[m, c] = result

            return carry

        lax.fori_loop(0, n_tp, part, 0)

    def pass_sum(m):
        for rel in range(1, chips):
            core_copy(m, rel).wait_recv()
            c = (chip + rel) % chips
            both = own_sum[m, c].astype(jnp.float32) + from_core[m, c].astype(jnp.float32)
            own_sum[m, c] = both.astype(jnp.bfloat16)
            chip_copy(m, rel).start()

    def total(m):
        owner, q = piece_at(m)
        core_copy(m, 0).wait_recv()
        value = own_sum[m, chip].astype(jnp.float32) + from_core[m, chip].astype(jnp.float32)
        for rel in range(1, chips):
            chip_copy(m, rel).wait_recv()
            value = value + from_chip[m, rel - 1].astype(jnp.float32)
        value = value.astype(out.dtype)
        if wide:
            for k, quarter in enumerate(weight_quarters(m, q)):
                to = pl.ds(pl.multiple_of(owner * cols_dev + quarter * col_w, col_w), col_w)
                out[:, to] = value[:, k * col_w : (k + 1) * col_w]
        else:
            out[:, pl.ds(pl.multiple_of(owner * cols_dev, cols_dev), cols_dev)] = value

    def piece(m, carry):
        multiply(m)
        pass_sum(m)

        @pl.when(m >= LAG)
        def _():
            total(m - LAG)

        return carry

    lax.fori_loop(0, 3 * nq, piece, 0)

    def out_step(s, last):
        for u in range(SUBS):
            ring_step(ow_ring, s, u, last)
            if (u + 1) % nr == 0:
                first = nq + (s - 1) * 2 * nq + 2 * (u // nr)
                lax.fori_loop(first, first + 2, piece, 0)

    def middle_out(s, carry):
        out_step(s, False)
        return carry

    lax.fori_loop(2, half - 1, middle_out, 0)
    out_step(half - 1, True)
    for k in range(SUBS // 2):
        ring_last(ow_ring, k)
        if wide:
            lax.fori_loop(pieces - nq + k, pieces - nq + k + 1, piece, 0)
    if not wide:
        lax.fori_loop(pieces - nq, pieces, piece, 0)

    def finish(m, carry):
        total(m)
        return carry

    lax.fori_loop(pieces - LAG, pieces, finish, 0)

    line_sent()
    ring_sent(ow_ring)
    for p in range(2):
        mate_weights(p).wait_send()

    def pair_sent(which):
        for j in range(CHUNKS):
            for copy in swap(0, j, which) + swap(1, j, which):
                copy.wait_send()
        for k in range(2):
            halo(k, which, 0).wait_send()

        @pl.when(pair < pairs - 1)
        def _():
            for k in range(2):
                halo(k, which, 1).wait_send()

        @pl.when(pair > 0)
        def _():
            for k in range(2):
                halo(k, which, 2).wait_send()

    each_member(pair_sent)

    def sums_sent(m, carry):
        core_copy(m, 0).wait_send()
        for rel in range(1, chips):
            core_copy(m, rel).wait_send()
            chip_copy(m, rel).wait_send()
        return carry

    lax.fori_loop(0, pieces, sums_sent, 0)


def shards(
    n_sp,
    n_tp,
    tokens,
    norm_gain,
    pool_in_weight,
    query_weight,
    key_weight,
    value_weight,
    pool_weight,
    pool_scale,
    sink_logit,
    out_pool_weight,
    out_attn_weight,
):
    rows, feats = tokens.shape
    depth, pool_ch = pool_in_weight.shape
    q_width = query_weight.shape[1]
    kvw = key_weight.shape[1]
    cols_dev = out_pool_weight.shape[1]
    pool_half, q_half = pool_ch // 2, q_width // 2
    out_rows = pool_ch + q_width
    half = n_sp // 2
    chips = n_tp // 2
    wide = cols_dev == SUBS * LANES
    nq = SUBS // 2 if wide else 1
    col_q = cols_dev // nq
    pieces = n_sp * nq
    part_rows = rows // n_tp
    kv_width = -(-kvw // LANES) * LANES
    in_cols = pool_half + q_half + kv_width
    if kv_width != kvw:
        key_weight, value_weight = (jnp.pad(w, ((0, 0), (0, kv_width - kvw))) for w in (key_weight, value_weight))
    tables = [jnp.asarray(t) for t in rotary_tables(rows * n_sp)]
    spread = jnp.asarray(spread_matrix(kvw // HEAD_DIM, kv_width), jnp.bfloat16)
    dims = dict(sp=n_sp, tp=n_tp, heads_kv=kvw // HEAD_DIM, nq=nq, wide=wide)
    small = (norm_gain.reshape(n_tp, 1, feats), pool_weight, pool_scale.reshape(1, pool_ch), *tables, spread)

    def kernel(*refs):
        layer_kernel(dims, *refs[:7], refs[7 : 7 + len(small)], *refs[7 + len(small) :])

    anywhere = pl.BlockSpec(memory_space=pl.ANY)
    vmem = pl.BlockSpec(memory_space=pltpu.VMEM)
    smem = pl.BlockSpec(memory_space=pltpu.SMEM)
    bf16, f32, dma = jnp.bfloat16, jnp.float32, pltpu.SemaphoreType.DMA
    return pl.pallas_call(
        kernel,
        out_shape=pltpu.VMEM((rows // n_tp, cols_dev * n_sp), bf16),
        in_specs=[anywhere] * (7 + len(small)) + [smem],
        out_specs=vmem,
        scratch_shapes=[
            pltpu.VMEM((2, n_tp, rows, feats), bf16),
            pltpu.VMEM((n_sp, depth, q_half + kv_width), bf16),
            pltpu.VMEM((n_sp, depth, pool_half), bf16),
            pltpu.VMEM((depth, q_half + kv_width), bf16),
            pltpu.VMEM((depth, pool_half), bf16),
            pltpu.VMEM((n_sp, SUBS if wide else 1, out_rows, LANES if wide else cols_dev), bf16),
            pltpu.VMEM((2, rows, in_cols), f32),
            pltpu.VMEM((2, rows, q_half), bf16),
            pltpu.VMEM((2, rows + 2 * POOL_PAD, pool_half), bf16),
            pltpu.VMEM((2, rows + 2 * WINDOW, kv_width), bf16),
            pltpu.VMEM((2, rows, pool_half), bf16),
            pltpu.VMEM((rows, q_half), bf16),
            pltpu.VMEM((2, rows, kv_width), bf16),
            pltpu.VMEM((rows + 2 * WINDOW, 4 * (kvw // HEAD_DIM) * LANES), bf16),
            pltpu.VMEM((rows, out_rows), bf16),
            pltpu.VMEM((pieces, chips, part_rows, col_q), bf16),
            pltpu.VMEM((pieces, chips, part_rows, col_q), bf16),
            pltpu.VMEM((pieces, chips, part_rows, col_q), bf16),
            pltpu.VMEM((pieces, chips - 1, part_rows, col_q), bf16),
            *[pltpu.VMEM(value.shape, value.dtype) for value in small],
            dma((7 + 2 * (SUBS if wide else 1) + len(small),)),
            dma((2,)),
            dma((2,)),
            dma((2, 2, half, 2)),
            dma((2, 2, half, 2)),
            dma((2, half, SUBS)),
            dma((2, half, SUBS)),
            dma((2, chips - 1, CHUNKS)),
            dma((2, chips - 1, CHUNKS)),
            dma((2, chips, CHUNKS)),
            dma((2, chips, CHUNKS)),
            dma((CHUNKS,)),
            dma((CHUNKS,)),
            dma((3, CHUNKS)),
            dma((3, CHUNKS)),
            dma((2, 2, 3)),
            dma((2, 2, 3)),
            dma((pieces, chips)),
            dma((pieces, chips)),
            dma((pieces, chips - 1)),
            dma((pieces, chips - 1)),
        ],
        compiler_params=pltpu.CompilerParams(
            collective_id=0, has_side_effects=True, vmem_limit_bytes=61 * 2**20
        ),
        name="layer",
    )(
        tokens,
        pool_in_weight,
        query_weight,
        key_weight,
        value_weight,
        out_pool_weight,
        out_attn_weight,
        *small,
        sink_logit,
    )


def solution(mesh):
    return jax.shard_map(
        functools.partial(shards, mesh.shape["sp"], mesh.shape["tp"]),
        mesh=mesh,
        in_specs=(
            P("sp", "tp"),
            P(),
            P("sp", "tp"),
            P("sp", "tp"),
            P("sp", "tp"),
            P("sp", "tp"),
            P("tp", None, None),
            P("tp"),
            P("tp"),
            P("tp", "sp"),
            P("tp", "sp"),
        ),
        out_specs=P(("sp", "tp"), None),
        check_vma=False,
    )
```
